32 devices in a mesh: ep: 4 (over y, x), tp: 8 (over z, core).
Axes of the slice: x: 2, y: 2, z: 4, core: 2. Of those that a mesh axis runs over, the one named last changes fastest.
Arguments:
- query_latent: bfloat16 [2048, 1024], P('ep'), may hold values from -6 to 6
- joint_latent: bfloat16 [2048, 512], P('ep'), may hold values from -6 to 6
- rotary_key: bfloat16 [2048, 32], P('ep'), may hold values from -60 to 60
- query_gain: float32 [1024], replicated, may hold values from 0.1 to 1.9
- joint_gain: float32 [512], replicated, may hold values from 0.1 to 1.9
- query_weight: bfloat16 [1024, 2048], P(None, 'tp'), may hold values from -0.1875 to 0.1875
- query_rotary: bfloat16 [1024, 1024], P(None, 'tp'), may hold values from -0.1875 to 0.1875
- key_weight: bfloat16 [512, 2048], P(None, 'tp'), may hold values from -0.25 to 0.25
- value_weight: bfloat16 [512, 2048], P(None, 'tp'), may hold values from -0.25 to 0.25
- output_weight: bfloat16 [2048, 2048], P('tp'), may hold values from -6 to 6
- expert_input: bfloat16 [2048, 2048], P('ep'), may hold values from -6 to 6
- expert_gain: float32 [2048], replicated, may hold values from 0.1 to 1.9
- routes: int32 [2048, 2], P('ep'), may hold values from 0 to 7, all different within a row; in each aligned block of 512 rows (0 to 511, 512 to 1023, ...) at most 192 rows name the same one
- route_weight: float32 [2048, 2], P('ep'), may hold values from 0.2 to 1
- gate_weight: bfloat16 [8, 2048, 4096], P('ep', None, 'tp'), may hold values from -0.125 to 0.125
- up_weight: bfloat16 [8, 2048, 4096], P('ep', None, 'tp'), may hold values from -0.125 to 0.125
- down_weight: bfloat16 [8, 4096, 2048], P('ep', 'tp'), may hold values from -0.09375 to 0.09375
Outputs:
- mixer_out: bfloat16 [2048, 2048], P(('ep', 'tp'))
- expert_out: bfloat16 [2048, 2048], P('ep', 'tp')
The draws below stay inside these ranges and needn't reach their ends.
Inputs may be any that keep to these rules, and one draw needn't show every extreme that they name: `routes`: A row names 2 different experts. Among the rows of one device (aligned blocks of 512 rows) no expert is named by more than 192 rows, a bound that some block reaches.
All inputs are finite; a program needn't handle non-finite values.
Results may differ from the reference program's by a relative error of at most 0.019.
The reference program's roundings to bfloat16 on the way count: a program that leaves them out, or rounds other values in their place, can miss the bound.
Values may be sent and summed in bfloat16 or wider, within the bound.
No kernel may reach another device: no remote copies, remote signals or barrier semaphores. Data moves between devices by JAX's collectives and lax.ppermute only.
A program may use at most 128 MiB of HBM per device.

```python
import math
import jax
import jax.numpy as jnp
import numpy as np
from jax import lax

D = 2048
HEADS = 32
NOPE = 64
ROPE = 32
VDIM = 64
QL = 1024
KVL = 512
FF = 4096
TOPK = 2
TOK_B_DEV = 512
EXPERTS = 8
TOK_A = 2048
TOK_B = 2048
CAP = 192
N_EP = 4
N_TP = 8


def draw_rotary_key(key, part):
    base = jax.random.normal(jax.random.fold_in(key, 11), (TOK_A, ROPE), jnp.float32)
    return jnp.clip(base, -60.0, 60.0).astype(jnp.bfloat16)


def level_of(stream_key, shape, shards, low, high):
    def one(dim, blocks):
        draws = jax.random.uniform(jax.random.fold_in(jax.random.fold_in(stream_key, 6), dim), (blocks,), jnp.float32, low / len(shards), high / len(shards))
        return jnp.repeat(jnp.exp(draws), shape[dim] // blocks).reshape((-1,) + (1,) * (len(shape) - dim - 1))

    gain = one(*shards[0])
    for cut in shards[1:]:
        gain = gain * one(*cut)
    return gain


def deal_out(rng, own, number, rows, amount, top, most, slope):
    sequence = jax.random.permutation(rng, amount)
    packed, usual = load_shares(amount, rows * top, most, slope, True), load_shares(amount, rows * top, most, slope, False)
    places = jnp.arange(amount)

    def named(sizes, rotation):
        used = int((sizes > 0).sum())
        fixed = max(1, used // 4)
        passed = fixed + (places - fixed + rotation * (used - fixed)) % max(1, amount - fixed)
        return jnp.zeros((amount,), jnp.int32).at[sequence[jnp.where(places < fixed, places, passed)]].set(jnp.asarray(sizes, jnp.int32))

    sizes = jnp.where(number % 4 == 0, named(packed, number // 4), named(usual, number - number // 4 - 1))
    mixed = jax.random.permutation(jax.random.fold_in(own, 3), amount)
    giver, receiver = mixed[0:amount // 2 * 2:2], mixed[1:amount // 2 * 2:2]
    margin = jnp.minimum(sizes[giver] - 1, most - sizes[receiver]) // 2
    margin = jnp.where((giver == sequence[0]) | (receiver == sequence[0]) | (sizes[receiver] == 0), 0, jnp.maximum(margin, 0))
    passed = jax.random.randint(jax.random.fold_in(own, 4), (amount // 2,), 0, 1 << 20) % (margin + 1)
    sizes = sizes.at[giver].add(-passed).at[receiver].add(passed)
    members = jnp.searchsorted(jnp.cumsum(sizes), jnp.arange(rows * top), side="right").astype(jnp.int32)
    listing = members.reshape(top, rows).T
    listing = listing[jax.random.permutation(jax.random.fold_in(own, 1), rows)]
    rotation = jax.random.randint(jax.random.fold_in(own, 2), (rows, 1), 0, top)
    return jnp.take_along_axis(listing, (jnp.arange(top)[None, :] + rotation) % top, axis=1)


def load_shares(count, total, reach, skew, full):
    weights = [(1 << 20) // math.isqrt(grade ** skew) + 1 for grade in range(1, count + 1)]
    largest = reach if full else min(reach, max(-(-total // count), total * weights[0] // sum(weights)))
    least = 1 if total - largest >= count - 1 else 0
    given, rest = [largest] + [least] * (count - 1), total - largest - least * (count - 1)
    while rest > 0:
        free = [i for i in range(1, count) if given[i] < largest] or [i for i in range(1, count) if given[i] < reach]
        mass, remaining = sum([weights[i] for i in free]), rest
        for i in free:
            addition = min(reach - given[i], max(1, remaining * weights[i] // mass), rest)
            given[i] = given[i] + addition
            rest = rest - addition
    return np.array(given)


def gaussian(stream_key, dims, scale, bound, cuts=(), kind=jnp.bfloat16):
    loudness = level_of(stream_key, dims, cuts, -0.22, 0.18) if cuts else 1.0
    result = jax.random.normal(stream_key, dims, jnp.float32) * scale * loudness
    return jnp.minimum(jnp.maximum(result, -bound), bound).astype(kind)


def setup_inputs(seed: int = 0) -> dict:
    keys = jax.random.split(jax.random.key(seed), 18)
    query_latent = gaussian(keys[0], (TOK_A, QL), 1.0, 6.0, ((0, 4),))
    joint_latent = gaussian(keys[1], (TOK_A, KVL), 1.0, 6.0, ((0, 4),))
    rotary_key = draw_rotary_key(jax.random.fold_in(keys[17], 71), 0)
    query_gain = jnp.clip(1.0 + 0.18 * jax.random.normal(keys[3], (QL,), jnp.float32), 0.1, 1.9)
    joint_gain = jnp.clip(1.0 + 0.18 * jax.random.normal(keys[4], (KVL,), jnp.float32), 0.1, 1.9)
    query_weight = gaussian(keys[5], (QL, HEADS * NOPE), QL ** -0.5, 0.1875, ((1, 8),))
    query_rotary = gaussian(keys[6], (QL, HEADS * ROPE), QL ** -0.5, 0.1875, ((1, 8),))
    key_weight = gaussian(keys[7], (KVL, HEADS * NOPE), KVL ** -0.5, 0.25, ((1, 8),))
    value_weight = gaussian(keys[8], (KVL, HEADS * VDIM), KVL ** -0.5, 0.25, ((1, 8),))
    output_weight = gaussian(keys[9], (HEADS * VDIM, D), 1.0, 6.0, ((0, 8),))
    expert_input = gaussian(keys[10], (TOK_B, D), 1.0, 6.0, ((0, 4),))
    expert_gain = jnp.clip(1.0 + 0.18 * jax.random.normal(keys[11], (D,), jnp.float32), 0.1, 1.9)
    routes_keys = jax.random.split(jax.random.fold_in(keys[12], 1), TOK_B // TOK_B_DEV)
    routes_turns = jax.random.permutation(jax.random.fold_in(keys[12], 3), TOK_B // TOK_B_DEV)
    routes = jax.vmap(lambda own, number: deal_out(jax.random.fold_in(keys[12], 2), own, number, TOK_B_DEV, EXPERTS, TOPK, CAP, 1))(routes_keys, routes_turns).reshape((TOK_B, TOPK))
    route_weight = jnp.clip(0.2 + 0.8 * jax.random.uniform(keys[13], (TOK_B, TOPK), jnp.float32) ** level_of(keys[13], (TOK_B, TOPK), ((0, 4),), -0.2, 0.2), 0.2, 1.0)
    gate_weight = gaussian(keys[14], (EXPERTS, D, FF), D ** -0.5, 0.125, ((0, 4), (2, 8)))
    up_weight = gaussian(keys[15], (EXPERTS, D, FF), D ** -0.5, 0.125, ((0, 4), (2, 8)))
    down_weight = gaussian(keys[16], (EXPERTS, FF, D), FF ** -0.5, 0.09375, ((0, 4), (1, 8)))
    return dict(query_latent=query_latent, joint_latent=joint_latent, rotary_key=rotary_key, query_gain=query_gain, joint_gain=joint_gain, query_weight=query_weight, query_rotary=query_rotary, key_weight=key_weight, value_weight=value_weight, output_weight=output_weight, expert_input=expert_input, expert_gain=expert_gain, routes=routes, route_weight=route_weight, gate_weight=gate_weight, up_weight=up_weight, down_weight=down_weight)


NORM_EPSILON = 1e-06
ROTARY_BASE = 10000.0

def norm_rows(source, gain_vector):
    as_float = source.astype(jnp.float32)
    factor = lax.rsqrt(lax.optimization_barrier(jnp.mean(as_float * as_float, axis=-1, keepdims=True)) + NORM_EPSILON)
    return (as_float * factor * gain_vector.astype(jnp.float32)).astype(jnp.bfloat16)

def rotate(source, positions):
    half_width = source.shape[-1] // 2
    frequencies = ROTARY_BASE ** (-jnp.arange(half_width, dtype=jnp.float32) / half_width)
    angles = positions[:, None] * frequencies[None, :]
    view_shape = (source.shape[0],) + (1,) * (source.ndim - 2) + (half_width,)
    cosine_table = jnp.cos(angles).reshape(view_shape)
    sine_table = jnp.sin(angles).reshape(view_shape)
    first_half = source[..., :half_width]
    second = source[..., half_width:]
    return jnp.concatenate([first_half * cosine_table - second * sine_table, second * cosine_table + first_half * sine_table], axis=-1)

def reference(query_latent, joint_latent, rotary_key, query_gain, joint_gain, query_weight, query_rotary, key_weight, value_weight, output_weight, expert_input, expert_gain, routes, route_weight, gate_weight, up_weight, down_weight):
    positions = jnp.arange(TOK_A, dtype=jnp.float32)
    query_normed = norm_rows(query_latent, query_gain)
    joint_normed = norm_rows(joint_latent, joint_gain)
    turned_key = rotate(rotary_key.astype(jnp.float32), positions).astype(jnp.bfloat16)
    query_plain = jnp.dot(query_normed, query_weight, preferred_element_type=jnp.float32).astype(jnp.bfloat16)
    query_plain = query_plain.reshape(TOK_A, HEADS, NOPE)
    query_turned = jnp.dot(query_normed, query_rotary, preferred_element_type=jnp.float32)
    query_turned = rotate(query_turned.reshape(TOK_A, HEADS, ROPE), positions).astype(jnp.bfloat16)
    key_plain = jnp.dot(joint_normed, key_weight, preferred_element_type=jnp.float32).astype(jnp.bfloat16)
    key_plain = key_plain.reshape(TOK_A, HEADS, NOPE)
    values = jnp.dot(joint_normed, value_weight, preferred_element_type=jnp.float32).astype(jnp.bfloat16)
    values = values.reshape(TOK_A, HEADS, VDIM)
    score_scale = (NOPE + ROPE) ** (-0.5)

    def one_head(items_in):
        query_head, turned_head, key_head, value_head = items_in
        scores = jnp.dot(query_head, key_head.T, preferred_element_type=jnp.float32)
        scores = (scores + jnp.dot(turned_head, turned_key.T, preferred_element_type=jnp.float32)) * score_scale
        row_top = lax.optimization_barrier(jnp.max(scores, axis=-1, keepdims=True))
        expo = jnp.exp(scores - row_top)
        row_total = lax.optimization_barrier(jnp.sum(expo, axis=-1, keepdims=True))
        mixed_values = jnp.dot(expo.astype(jnp.bfloat16), value_head, preferred_element_type=jnp.float32)
        return (mixed_values / row_total).astype(jnp.bfloat16)
    per_head = lax.map(one_head, (query_plain.transpose(1, 0, 2), query_turned.transpose(1, 0, 2), key_plain.transpose(1, 0, 2), values.transpose(1, 0, 2)))
    attended = per_head.transpose(1, 0, 2).reshape(TOK_A, HEADS * VDIM)
    mixer_out = jnp.dot(attended, output_weight, preferred_element_type=jnp.float32).astype(jnp.bfloat16)
    expert_normed = norm_rows(expert_input, expert_gain)
    flat_routes = routes.reshape(-1).astype(jnp.int32)
    pair_count = TOK_B * TOPK
    owner_token = jnp.arange(pair_count, dtype=jnp.int32) // TOPK
    onehot = (flat_routes[:, None] == jnp.arange(EXPERTS, dtype=jnp.int32)[None, :]).astype(jnp.int32)
    rank_within = lax.optimization_barrier(jnp.sum((jnp.cumsum(onehot, axis=0) - onehot) * onehot, axis=1)).astype(jnp.int32)
    slot_width = N_EP * CAP
    slot_token = jnp.zeros((EXPERTS, slot_width), jnp.int32).at[flat_routes, rank_within].set(owner_token)
    block_width = FF // N_TP

    def one_expert(items_in):
        token_index, gate_matrix, up_matrix, down_matrix = items_in
        rows_in = expert_normed[token_index]
        gate_acts = jnp.dot(rows_in, gate_matrix, preferred_element_type=jnp.float32)
        up_acts = jnp.dot(rows_in, up_matrix, preferred_element_type=jnp.float32)
        hidden = (jax.nn.silu(gate_acts) * up_acts).astype(jnp.bfloat16)

        def add_block(running, block_index):
            start_at = (block_index * block_width).astype(jnp.int32)
            part_sum = jnp.dot(lax.dynamic_slice_in_dim(hidden, start_at, block_width, 1), lax.dynamic_slice_in_dim(down_matrix, start_at, block_width, 0), preferred_element_type=jnp.float32)
            part_sum = lax.optimization_barrier(part_sum.astype(jnp.bfloat16))
            return (running + part_sum.astype(jnp.float32), None)
        running, _ = lax.scan(add_block, jnp.zeros((slot_width, D), jnp.float32), jnp.arange(N_TP, dtype=jnp.int32))
        return running.astype(jnp.bfloat16)
    results = lax.map(one_expert, (slot_token, gate_weight, up_weight, down_weight))
    picked = results[flat_routes, rank_within].astype(jnp.float32).reshape(TOK_B, TOPK, D)
    expert_out = lax.optimization_barrier(jnp.sum(picked * route_weight[:, :, None], axis=1)).astype(jnp.bfloat16)
    return (mixer_out, expert_out)
```

```python
import functools

import jax
import jax.numpy as jnp
from jax import lax
from jax.experimental import pallas as pl
from jax.experimental.pallas import tpu as pltpu
from jax.sharding import PartitionSpec as P

NOPE = 64
VDIM = 64
NORM_EPSILON = 1e-06
ROTARY_BASE = 10000.0
LOG2E = 1.4426950408889634

F32 = jnp.float32
BF16 = jnp.bfloat16
VMEM_LIMIT = 56 * 1024 * 1024


SMEM_SPEC = pl.BlockSpec(memory_space=pltpu.SMEM)
VMEM_SPEC = pl.BlockSpec(memory_space=pltpu.VMEM)
ANY_SPEC = pl.BlockSpec(memory_space=pl.ANY)


def params():
    return pltpu.CompilerParams(vmem_limit_bytes=VMEM_LIMIT)


def cost(flops, bytes_accessed):
    return pl.CostEstimate(
        flops=int(flops), bytes_accessed=int(bytes_accessed), transcendentals=0
    )


def swap_over(value, axis, mask):
    size = lax.axis_size(axis)
    return lax.ppermute(value, axis, [(i, i ^ mask) for i in range(size)])


def bits_of(size):
    return max(size - 1, 0).bit_length()


def spread(index, bits):
    return sum(((index >> (bits - 1 - b)) & 1) << b for b in range(bits))


def norm_value(source, gain):
    wide = source.astype(F32)
    factor = lax.rsqrt(jnp.mean(wide * wide, axis=-1, keepdims=True) + NORM_EPSILON)
    return (wide * factor * gain).astype(BF16)


def rotate_lanes(source, cosine, sine, half):
    width = source.shape[-1]
    lane = lax.broadcasted_iota(jnp.int32, source.shape, 1)
    first = (lane & (2 * half - 1)) < half
    partner = jnp.where(
        first, pltpu.roll(source, width - half, 1), pltpu.roll(source, half, 1)
    )
    return source * cosine + partner * sine


def rows_norm_kernel(ids, source, gain, mine, other):
    half = mine.shape[0]
    core = ids[1]
    own = pl.multiple_of(core * half, half)
    far = pl.multiple_of((1 - core) * half, half)
    mine[...] = norm_value(source[pl.ds(own, half), :], gain[...])
    other[...] = norm_value(source[pl.ds(far, half), :], gain[...])


def rows_norm(ids, source, gain):
    rows, width = source.shape
    shape = jax.ShapeDtypeStruct((rows // 2, width), BF16)
    return pl.pallas_call(
        rows_norm_kernel,
        out_shape=(shape, shape),
        in_specs=[SMEM_SPEC, VMEM_SPEC, VMEM_SPEC],
        out_specs=(VMEM_SPEC, VMEM_SPEC),
        compiler_params=params(),
        cost_estimate=cost(2000 * rows * width, 4 * rows * width),
        name="rows_norm",
    )(ids, source, gain.reshape(1, width))


def latent_kernel(turn, ids, source, gain, rotary, cosine, sine, mine, other):
    half, full = mine.shape
    width = source.shape[1]
    repeat = (full - width) // rotary.shape[1]
    core = ids[1]
    for target, start in ((mine, core * half), (other, (1 - core) * half)):
        rows = pl.ds(pl.multiple_of(start, half), half)
        target[:, :width] = norm_value(source[rows, :], gain[...])
        key = rotary[rows, :].astype(F32)
        key = jnp.concatenate([key] * repeat, axis=1) if repeat > 1 else key
        target[:, width:] = rotate_lanes(
            key, cosine[rows, :], sine[rows, :], turn
        ).astype(BF16)


def latent_pack(ids, source, gain, rotary, cosine, sine):
    rows, width = source.shape
    turned = cosine.shape[1]
    shape = jax.ShapeDtypeStruct((rows // 2, width + turned), BF16)
    return pl.pallas_call(
        functools.partial(latent_kernel, rotary.shape[1] // 2),
        out_shape=(shape, shape),
        in_specs=[SMEM_SPEC] + [VMEM_SPEC] * 5,
        out_specs=(VMEM_SPEC, VMEM_SPEC),
        compiler_params=params(),
        cost_estimate=cost(2000 * rows * width, 4 * rows * width),
        name="latent_pack",
    )(ids, source, gain.reshape(1, width), rotary, cosine, sine)


def attention_kernel(
    turn_width, piece_count, tp_bits, ids, query_latent, gain, query_weight, query_rotary,
    cosine, sine, key_weight, value_weight, output_weight, *rest
):
    pieces = rest[:piece_count]
    keep, send, plain, turned, keys, values, mixed = rest[piece_count:]
    rows = query_latent.shape[0]
    latent = key_weight.shape[0]
    turn_lanes = cosine.shape[1]
    pair_count = keys.shape[0]
    pair = 2 * NOPE
    scale = LOG2E * (NOPE + turn_width) ** (-0.5)

    normed = norm_value(query_latent[...], gain[...])
    plain[...] = jnp.dot(normed, query_weight[...], preferred_element_type=F32).astype(BF16)
    turned[...] = rotate_lanes(
        jnp.dot(normed, query_rotary[...], preferred_element_type=F32),
        cosine[...],
        sine[...],
        turn_width // 2,
    ).astype(BF16)

    start = 0
    for piece in pieces:
        count = piece.shape[0]
        block = piece[:, :latent]
        key_block = jnp.dot(block, key_weight[...], preferred_element_type=F32).astype(BF16)
        value_block = jnp.dot(block, value_weight[...], preferred_element_type=F32).astype(BF16)
        for p in range(pair_count):
            keys[p, start : start + count, :pair] = key_block[:, p * pair : (p + 1) * pair]
            keys[p, start : start + count, pair:] = piece[:, latent:]
            values[p, start : start + count, :] = value_block[:, p * pair : (p + 1) * pair]
        start += count

    tile = min(rows, 256)
    plain_lane = lax.broadcasted_iota(jnp.int32, (tile, pair), 1)
    turn_lane = lax.broadcasted_iota(jnp.int32, (tile, turn_lanes), 1)
    zero = jnp.zeros((), BF16)

    def step(index, carry):
        row = pl.ds(pl.multiple_of(index * tile, tile), tile)
        for p in range(pair_count):
            outs = []
            for h in range(2):
                head = 2 * p + h
                left = jnp.where(
                    (plain_lane // NOPE) == h, plain[row, p * pair : (p + 1) * pair], zero
                )
                right = jnp.where((turn_lane // turn_width) == head, turned[row, :], zero)
                query = jnp.concatenate([left, right], axis=1)
                scores = lax.dot_general(
                    query, keys[p], (((1,), (1,)), ((), ())), preferred_element_type=F32
                )
                top = jnp.max(scores, axis=1, keepdims=True)
                expo = jnp.exp2((scores - top) * scale)
                total = jnp.sum(expo, axis=1, keepdims=True)
                mix = jnp.dot(expo.astype(BF16), values[p], preferred_element_type=F32)
                outs.append(mix / total)
            mixed[row, p * pair : (p + 1) * pair] = jnp.where(
                plain_lane < VDIM, outs[0], outs[1]
            ).astype(BF16)
        return carry

    lax.fori_loop(0, rows // tile, step, 0)

    place_count = 1 << tp_bits
    block_rows = rows // place_count
    me = ids[0]
    half = place_count // 2
    for target, low in ((keep, 0), (send, half)):
        parts = [
            mixed[
                pl.ds(
                    pl.multiple_of((me ^ spread(low + i, tp_bits)) * block_rows, block_rows),
                    block_rows,
                ),
                :,
            ]
            for i in range(half)
        ]
        target[...] = jnp.dot(
            jnp.concatenate(parts, axis=0), output_weight[...], preferred_element_type=F32
        ).astype(BF16)


def attention(
    ids, query_latent, gain, query_weight, query_rotary, cosine, sine, key_weight,
    value_weight, output_weight, pieces, turn_width, tp_bits,
):
    rows, query_width = query_latent.shape
    head_count = key_weight.shape[1] // NOPE
    key_rows = sum(p.shape[0] for p in pieces)
    turn_lanes = cosine.shape[1]
    width = output_weight.shape[1]
    shape = jax.ShapeDtypeStruct((rows // 2, width), BF16)
    return pl.pallas_call(
        functools.partial(attention_kernel, turn_width, len(pieces), tp_bits),
        out_shape=(shape, shape),
        in_specs=[SMEM_SPEC] + [VMEM_SPEC] * (9 + len(pieces)),
        out_specs=(VMEM_SPEC, VMEM_SPEC),
        scratch_shapes=[
            pltpu.VMEM((rows, head_count * NOPE), BF16),
            pltpu.VMEM((rows, turn_lanes), BF16),
            pltpu.VMEM((head_count // 2, key_rows, 2 * NOPE + turn_lanes), BF16),
            pltpu.VMEM((head_count // 2, key_rows, 2 * VDIM), BF16),
            pltpu.VMEM((rows, head_count * VDIM), BF16),
        ],
        compiler_params=params(),
        cost_estimate=cost(4e12 * 12e-6, 8e6),
        name="attention",
    )(
        ids, query_latent, gain.reshape(1, query_width), query_weight, query_rotary, cosine,
        sine, key_weight, value_weight, output_weight, *pieces
    )


def experts_kernel(
    block_pieces, capacity, tp_bits, ids, gate_hbm, up_hbm, down_hbm, *rest
):
    blocks = len(block_pieces)
    metas = rest[:blocks]
    pieces = rest[blocks : blocks + sum(block_pieces)]
    keep, send, gate, up, down, slots, loads, gathered, sems = rest[blocks + sum(block_pieces) :]
    local_count = gate.shape[0]
    tokens = metas[0].shape[1]
    half = tokens // 2
    me, core, group = ids[0], ids[1], ids[2]

    copies = []
    for j in range(local_count):
        trio = []
        for k, (source, target) in enumerate(((gate_hbm, gate), (up_hbm, up), (down_hbm, down))):
            copy = pltpu.make_async_copy(source.at[j], target.at[j], sems.at[j, k])
            copy.start()
            trio.append(copy)
        copies.append(trio)

    before = (
        lax.broadcasted_iota(jnp.int32, (tokens, tokens), 0)
        < lax.broadcasted_iota(jnp.int32, (tokens, tokens), 1)
    ).astype(BF16)
    row = lax.broadcasted_iota(jnp.int32, (8, tokens), 0)
    wanted = (row + group * local_count).astype(F32)
    for b in range(blocks):
        meta = metas[b][...]
        first = meta[0:1, :] == wanted
        second = meta[1:2, :] == wanted
        named = (first | second) & (row < local_count)
        rank = jnp.dot(named.astype(BF16), before, preferred_element_type=F32)
        slots[b] = jnp.where(named, rank, -1.0)
        loads[b] = jnp.where(first, meta[2:3, :], 0.0) + jnp.where(second, meta[3:4, :], 0.0)

    own = pl.multiple_of(core * half, half)
    far = pl.multiple_of((1 - core) * half, half)
    place = lax.broadcasted_iota(jnp.int32, (capacity, half), 0).astype(F32)
    place_count = 1 << tp_bits
    part = down.shape[2] // place_count
    scales = []
    for j in range(local_count):
        scale = []
        start = 0
        for b in range(blocks):
            count = block_pieces[b] // 2
            total = None
            weight = None
            for side, offset in ((0, own), (1, far)):
                hit = place == slots[b, j : j + 1, pl.ds(offset, half)]
                load = jnp.where(hit, loads[b, j : j + 1, pl.ds(offset, half)], 0.0)
                load = jnp.sum(load, axis=1, keepdims=True)
                refs = pieces[start + side * count : start + (side + 1) * count]
                block = [r[...] for r in refs]
                block = jnp.concatenate(block, axis=0) if count > 1 else block[0]
                found = jnp.dot(
                    jnp.where(hit, 1.0, 0.0).astype(BF16), block, preferred_element_type=F32
                )
                total = found if total is None else total + found
                weight = load if weight is None else weight + load
            gathered[j, b * capacity : (b + 1) * capacity, :] = total.astype(BF16)
            scale.append(weight)
            start += block_pieces[b]
        scales.append(scale)

    for j in range(local_count):
        rows_in = gathered[j]
        copies[j][0].wait()
        gate_acts = jnp.dot(rows_in, gate[j], preferred_element_type=F32)
        copies[j][1].wait()
        up_acts = jnp.dot(rows_in, up[j], preferred_element_type=F32)
        hidden = (gate_acts * (1.0 / (1.0 + jnp.exp(-gate_acts))) * up_acts).astype(BF16)
        copies[j][2].wait()
        for target, low in ((send, place_count // 2), (keep, 0)):
            for i in range(place_count // 2):
                column = pl.multiple_of((me ^ spread(low + i, tp_bits)) * part, part)
                product = jnp.dot(
                    hidden, down[j, :, pl.ds(column, part)], preferred_element_type=F32
                )
                for b in range(blocks):
                    base = (b * local_count + j) * capacity
                    target[base : base + capacity, i * part : (i + 1) * part] = (
                        product[b * capacity : (b + 1) * capacity, :] * scales[j][b]
                    ).astype(BF16)


def run_experts(ids, metas, blocks, gate_weight, up_weight, down_weight, capacity, tp_bits):
    local_count, width, hidden = gate_weight.shape
    count = len(blocks)
    tokens = metas[0].shape[1]
    flat = [p for block in blocks for p in block]
    rows = count * local_count * capacity
    shape = jax.ShapeDtypeStruct((rows, width // 2), BF16)
    return pl.pallas_call(
        functools.partial(
            experts_kernel, tuple(len(block) for block in blocks), capacity, tp_bits
        ),
        out_shape=(shape, shape),
        in_specs=[SMEM_SPEC] + [ANY_SPEC] * 3 + [VMEM_SPEC] * (count + len(flat)),
        out_specs=(VMEM_SPEC, VMEM_SPEC),
        scratch_shapes=[
            pltpu.VMEM(gate_weight.shape, BF16),
            pltpu.VMEM(up_weight.shape, BF16),
            pltpu.VMEM(down_weight.shape, BF16),
            pltpu.VMEM((count, 8, tokens), F32),
            pltpu.VMEM((count, 8, tokens), F32),
            pltpu.VMEM((local_count, count * capacity, width), BF16),
            pltpu.SemaphoreType.DMA((local_count, 3)),
        ],
        compiler_params=params(),
        cost_estimate=cost(4e12 * 5e-6 * count, 12e6),
        name="experts",
    )(ids, gate_weight, up_weight, down_weight, *metas, *flat)


def combine_kernel(local_count, capacity, group_count, with_carry, ids, routes, *rest):
    parts = rest[:group_count]
    carry = rest[group_count] if with_carry else None
    outs = rest[group_count + int(with_carry) :]
    tokens = routes.shape[0]
    group = ids[2]
    lanes = max(128, group_count * local_count)
    lane = lax.broadcasted_iota(jnp.int32, (tokens, lanes), 1)
    expert = (group ^ (lane // local_count)) * local_count + lane % local_count
    live = lane < group_count * local_count
    first = (routes[:, 0:1] == expert) & live
    second = (routes[:, 1:2] == expert) & live
    before = (
        lax.broadcasted_iota(jnp.int32, (tokens, tokens), 1)
        < lax.broadcasted_iota(jnp.int32, (tokens, tokens), 0)
    ).astype(BF16)
    named = jnp.where(first | second, 1.0, 0.0).astype(BF16)
    slot = jnp.dot(before, named, preferred_element_type=F32) + (lane * capacity).astype(F32)
    slot_first = jnp.sum(jnp.where(first, slot, 0.0), axis=1, keepdims=True)
    slot_second = jnp.sum(jnp.where(second, slot, 0.0), axis=1, keepdims=True)
    span = local_count * capacity
    total = None
    for r in range(group_count):
        place = (lax.broadcasted_iota(jnp.int32, (tokens, span), 1) + r * span).astype(F32)
        pick = jnp.where((place == slot_first) | (place == slot_second), 1.0, 0.0).astype(BF16)
        found = jnp.dot(pick, parts[r][...], preferred_element_type=F32)
        total = found if total is None else total + found
    if with_carry:
        total = total + carry[...].astype(F32)
    start = 0
    for out in outs:
        out[...] = total[:, start : start + out.shape[1]].astype(BF16)
        start += out.shape[1]


def combine(ids, routes, parts, carry, widths, local_count, capacity):
    tokens = routes.shape[0]
    operands = list(parts) + ([] if carry is None else [carry])
    return pl.pallas_call(
        functools.partial(
            combine_kernel, local_count, capacity, len(parts), carry is not None
        ),
        out_shape=tuple(jax.ShapeDtypeStruct((tokens, w), BF16) for w in widths),
        in_specs=[SMEM_SPEC] + [VMEM_SPEC] * (1 + len(operands)),
        out_specs=tuple(VMEM_SPEC for _ in widths),
        compiler_params=params(),
        cost_estimate=cost(4e12 * 3e-6, 4e6),
        name="combine",
    )(ids, routes, *operands)


def low_bit(value):
    return value & -value


def high_bit(value):
    return 1 << (value.bit_length() - 1)


def gather_halves(mine, group_count):
    rows = mine.shape[0]
    pieces = (mine[: rows // 2], mine[rows // 2 :])
    held = {0: pieces}
    for weight in range(1, bits_of(group_count) + 1):
        for r in range(1, group_count):
            if bin(r).count("1") != weight:
                continue
            low, high = low_bit(r), high_bit(r)
            held[r] = (
                swap_over(held[r ^ high][0], "ep", high),
                swap_over(held[r ^ low][1], "ep", low),
            )
    return held


def add_wide(left, right):
    return (left.astype(F32) + right.astype(F32)).astype(BF16)


def local(
    query_latent,
    joint_latent,
    rotary_key,
    query_gain,
    joint_gain,
    query_weight,
    query_rotary,
    key_weight,
    value_weight,
    output_weight,
    expert_input,
    expert_gain,
    routes,
    route_weight,
    gate_weight,
    up_weight,
    down_weight,
):
    group_count = lax.axis_size("ep")
    part_count = lax.axis_size("tp")
    ep_bits, tp_bits = bits_of(group_count), bits_of(part_count)
    ep, tp = lax.axis_index("ep"), lax.axis_index("tp")
    ids = jnp.stack([tp, tp & 1, ep]).astype(jnp.int32)
    rows = query_latent.shape[0]
    turn_width = rotary_key.shape[1]
    head_count = key_weight.shape[1] // NOPE
    turn_lanes = head_count * turn_width
    local_count = gate_weight.shape[0]
    tokens = expert_input.shape[0]
    capacity = 3 * tokens // (2 * group_count)

    lane = jnp.arange(turn_lanes, dtype=jnp.int32)
    half_width = turn_width // 2
    positions = (ep * rows + jnp.arange(rows, dtype=jnp.int32)).astype(F32)
    frequencies = ROTARY_BASE ** (-(lane % half_width).astype(F32) / half_width)
    angles = positions[:, None] * frequencies[None, :]
    cosine = jnp.cos(angles)
    sine = jnp.where((lane % turn_width)[None, :] < half_width, -jnp.sin(angles), jnp.sin(angles))

    latent_mine, latent_other = latent_pack(
        ids, joint_latent, joint_gain, rotary_key, cosine, sine
    )
    row_mine, row_other = rows_norm(ids, expert_input, expert_gain)
    meta = jnp.concatenate(
        [
            routes.astype(F32).T,
            route_weight.T,
            jnp.zeros((8 - 2 * routes.shape[1], tokens), F32),
        ],
        axis=0,
    )
    metas = {r: swap_over(meta, "ep", r) if r else meta for r in range(group_count)}
    latent_held = gather_halves(latent_mine, group_count)
    row_held = gather_halves(row_mine, group_count)

    pieces = [latent_mine, latent_other]
    for r in range(1, group_count):
        for piece in latent_held[r]:
            pieces += [piece, swap_over(piece, "tp", 1)]
    keep, send = attention(
        ids, query_latent, query_gain, query_weight, query_rotary, cosine, sine, key_weight,
        value_weight, output_weight, pieces, turn_width, tp_bits,
    )
    arrived = swap_over(send, "tp", 1)
    for b in range(1, tp_bits):
        cut = keep.shape[0] // 2
        away = add_wide(keep[cut:], arrived[cut:])
        keep = add_wide(keep[:cut], arrived[:cut])
        arrived = swap_over(away, "tp", 1 << b)
    mixer_out = add_wide(keep, arrived)

    parts = {}
    span = local_count * capacity
    for weight in range(ep_bits + 1):
        chosen = [r for r in range(group_count) if bin(r).count("1") == weight]
        blocks = []
        for r in chosen:
            if r == 0:
                blocks.append([row_mine, row_other])
            else:
                mine = list(row_held[r])
                blocks.append(mine + [swap_over(p, "tp", 1) for p in mine])
        keep, send = run_experts(
            ids, [metas[r] for r in chosen], blocks, gate_weight, up_weight, down_weight,
            capacity, tp_bits,
        )
        arrived = swap_over(send, "tp", 1)
        cut = keep.shape[1] // 2
        for i, r in enumerate(chosen):
            here = slice(i * span, (i + 1) * span)
            parts[r] = (
                add_wide(keep[here, :cut], arrived[here, :cut]),
                add_wide(keep[here, cut:], arrived[here, cut:]),
            )
    last = [
        swap_over(parts[r][1], "ep", r) if r else parts[r][1] for r in range(group_count)
    ]
    first = [
        swap_over(parts[r][0], "ep", r) if r else parts[r][0] for r in range(group_count)
    ]
    width = last[0].shape[1]
    (away,) = combine(ids, routes, last, None, (width,), local_count, capacity)
    arrived = swap_over(away, "tp", 2)
    if tp_bits == 2:
        (expert_out,) = combine(ids, routes, first, arrived, (width,), local_count, capacity)
    else:
        keep, away = combine(
            ids, routes, first, arrived, (width // 2, width // 2), local_count, capacity
        )
        arrived = swap_over(away, "tp", 4)
        for b in range(3, tp_bits):
            cut = keep.shape[1] // 2
            away = add_wide(keep[:, cut:], arrived[:, cut:])
            keep = add_wide(keep[:, :cut], arrived[:, :cut])
            arrived = swap_over(away, "tp", 1 << b)
        expert_out = add_wide(keep, arrived)
    return (mixer_out, expert_out)


def solution(mesh):
    return jax.shard_map(
        local,
        mesh=mesh,
        in_specs=(
            P("ep", None),
            P("ep", None),
            P("ep", None),
            P(),
            P(),
            P(None, "tp"),
            P(None, "tp"),
            P(None, "tp"),
            P(None, "tp"),
            P("tp", None),
            P("ep", None),
            P(),
            P("ep", None),
            P("ep", None),
            P("ep", None, "tp"),
            P("ep", None, "tp"),
            P("ep", "tp", None),
        ),
        out_specs=(P(("ep", "tp"), None), P("ep", "tp")),
        check_vma=False,
    )
```

```python
import functools

import jax
import jax.numpy as jnp
from jax import lax
from jax.experimental import pallas as pl
from jax.experimental.pallas import tpu as pltpu
from jax.sharding import PartitionSpec as P


NOPE = 64
VDIM = 64
NORM_EPSILON = 1e-06
ROTARY_BASE = 10000.0
LOG2E = 1.4426950408889634

F32 = jnp.float32
BF16 = jnp.bfloat16

SMEM_SPEC = pl.BlockSpec(memory_space=pltpu.SMEM)
VMEM_SPEC = pl.BlockSpec(memory_space=pltpu.VMEM)
HBM_SPEC = pl.BlockSpec(memory_space=pltpu.HBM)


def params(mebibytes):
    return pltpu.CompilerParams(vmem_limit_bytes=mebibytes * 1024 * 1024)


def cost(flops, bytes_accessed):
    return pl.CostEstimate(
        flops=int(flops), bytes_accessed=int(bytes_accessed), transcendentals=0
    )


def swap_over(value, axis, mask):
    size = lax.axis_size(axis)
    return lax.ppermute(value, axis, [(i, i ^ mask) for i in range(size)])


def bits_of(size):
    return max(size - 1, 0).bit_length()


def spread(index, bits):
    return sum(((index >> (bits - 1 - b)) & 1) << b for b in range(bits))


def norm_value(source, gain):
    wide = source.astype(F32)
    factor = lax.rsqrt(jnp.mean(wide * wide, axis=-1, keepdims=True) + NORM_EPSILON)
    return (wide * factor * gain).astype(BF16)


def rotate_lanes(source, cosine, sine, half):
    width = source.shape[-1]
    lane = lax.broadcasted_iota(jnp.int32, source.shape, 1)
    first = (lane & (2 * half - 1)) < half
    partner = jnp.where(
        first, pltpu.roll(source, width - half, 1), pltpu.roll(source, half, 1)
    )
    return source * cosine + partner * sine


def prepare_kernel(
    ids, joint_hbm, joint_gain_hbm, rotary_hbm, routes_hbm, weights_hbm, rows_hbm, rows_gain_hbm,
    mine_hbm, other_hbm, meta_hbm, row_mine_hbm, row_other_hbm,
    joint, joint_gain, rotary, routes, weights, rows, rows_gain,
    mine, other, meta, row_mine, row_other, sems,
):
    inputs = (
        (joint_hbm, joint), (joint_gain_hbm, joint_gain), (rotary_hbm, rotary),
        (routes_hbm, routes), (weights_hbm, weights), (rows_gain_hbm, rows_gain), (rows_hbm, rows),
    )
    loads = [
        pltpu.make_async_copy(source, target, sems.at[i])
        for i, (source, target) in enumerate(inputs)
    ]
    outputs = (
        (mine, mine_hbm), (other, other_hbm), (meta, meta_hbm), (row_mine, row_mine_hbm),
        (row_other, row_other_hbm),
    )
    stores = [
        pltpu.make_async_copy(source, target, sems.at[len(loads) + i])
        for i, (source, target) in enumerate(outputs)
    ]
    for load in loads:
        load.start()
    for load in loads[:5]:
        load.wait()
    half, full = mine.shape
    count, width = joint.shape
    turn, top = rotary.shape[0], routes.shape[0]
    weight = weights[...]
    high = weight.astype(BF16).astype(F32)
    middle = (weight - high).astype(BF16).astype(F32)
    low = weight - high - middle
    rest = jnp.zeros((full - width - turn - 4 * top, count), F32)
    named = routes[...].astype(F32)
    meta[...] = jnp.concatenate([named, weight, rest[: 8 - 2 * top]], axis=0)
    side = jnp.concatenate(
        [rotary[...].astype(F32), named, high, middle, low, rest], axis=0
    ).T.astype(BF16)
    chosen = ids[1] == 0
    mine[:, width:] = jnp.where(chosen, side[:half], side[half:])
    other[:, width:] = jnp.where(chosen, side[half:], side[:half])
    own = pl.multiple_of(ids[1] * half, half)
    far = pl.multiple_of((1 - ids[1]) * half, half)
    mine[:, :width] = norm_value(joint[pl.ds(own, half), :], joint_gain[...])
    stores[0].start()
    other[:, :width] = norm_value(joint[pl.ds(far, half), :], joint_gain[...])
    stores[1].start()
    stores[2].start()
    for load in loads[5:]:
        load.wait()
    row_mine[...] = norm_value(rows[pl.ds(own, half), :], rows_gain[...])
    stores[3].start()
    row_other[...] = norm_value(rows[pl.ds(far, half), :], rows_gain[...])
    stores[4].start()
    for store in stores:
        store.wait()


def prepare(ids, joint, joint_gain, rotary, routes, weights, rows, rows_gain):
    count, width = joint.shape
    half = count // 2
    inputs = (
        joint, joint_gain.reshape(1, width), rotary.T, routes.T, weights.T, rows,
        rows_gain.reshape(1, rows.shape[1]),
    )
    outputs = (
        jax.ShapeDtypeStruct((half, width + 128), BF16),
        jax.ShapeDtypeStruct((half, width + 128), BF16),
        jax.ShapeDtypeStruct((8, count), F32),
        jax.ShapeDtypeStruct((half, rows.shape[1]), BF16),
        jax.ShapeDtypeStruct((half, rows.shape[1]), BF16),
    )
    return pl.pallas_call(
        prepare_kernel,
        out_shape=outputs,
        in_specs=[SMEM_SPEC] + [HBM_SPEC] * len(inputs),
        out_specs=(HBM_SPEC,) * len(outputs),
        scratch_shapes=[pltpu.VMEM(v.shape, v.dtype) for v in inputs + outputs]
        + [pltpu.SemaphoreType.DMA((len(inputs) + len(outputs),))],
        compiler_params=params(60),
        cost_estimate=cost(4e12 * 3e-6, 4e6),
        name="prepare",
    )(ids, *inputs)


def turn_tables(cosine, sine, start, count, lanes):
    turned = pl.ds(start, count)
    half = cosine.shape[0]
    repeat = lanes // (2 * half)
    c, s = cosine[:, turned], sine[:, turned]
    return (
        jnp.concatenate([c, c] * repeat, axis=0).T,
        jnp.concatenate([-s, s] * repeat, axis=0).T,
    )


def pick_value(local_count, capacity, group_count, ids, routes, out):
    tokens = routes.shape[1]
    group = ids[2]
    total = group_count * local_count
    row = lax.broadcasted_iota(jnp.int32, (total, tokens), 0)
    expert = ((group ^ (row // local_count)) * local_count + row % local_count)
    first = routes[0:1, :] == expert
    second = routes[1:2, :] == expert
    before = (
        lax.broadcasted_iota(jnp.int32, (tokens, tokens), 0)
        < lax.broadcasted_iota(jnp.int32, (tokens, tokens), 1)
    ).astype(BF16)
    named = jnp.where(first | second, 1.0, 0.0).astype(BF16)
    slot = jnp.dot(named, before, preferred_element_type=F32) + (row * capacity).astype(F32)
    pair = jnp.concatenate(
        [
            jnp.sum(jnp.where(first, slot, 0.0), axis=0, keepdims=True),
            jnp.sum(jnp.where(second, slot, 0.0), axis=0, keepdims=True),
            jnp.zeros((126, tokens), F32),
        ],
        axis=0,
    ).T
    span = 128
    for start in range(0, total * capacity, span):
        place = (lax.broadcasted_iota(jnp.int32, (tokens, span), 1) + start).astype(F32)
        out[:, start : start + span] = jnp.where(
            (place == pair[:, 0:1]) | (place == pair[:, 1:2]), 1.0, 0.0
        ).astype(BF16)


def query_kernel(
    turn_width, local_count, capacity, group_count, ids, query_latent, gain, query_weight,
    query_rotary, cosine, sine, routes, plain, turned, pick
):
    rows = query_latent.shape[0]
    normed = norm_value(query_latent[...], gain[...])
    plain[...] = jnp.dot(normed, query_weight[...], preferred_element_type=F32).astype(BF16)
    start = pl.multiple_of(ids[2] * rows, rows)
    c, s = turn_tables(cosine, sine, start, rows, turned.shape[1])
    turned[...] = rotate_lanes(
        jnp.dot(normed, query_rotary[...], preferred_element_type=F32), c, s, turn_width // 2
    ).astype(BF16)
    pick_value(local_count, capacity, group_count, ids, routes, pick)


def queries(
    ids, query_latent, gain, query_weight, query_rotary, cosine, sine, routes, turn_width,
    local_count, capacity, group_count,
):
    rows, width = query_latent.shape
    tokens = routes.shape[0]
    return pl.pallas_call(
        functools.partial(query_kernel, turn_width, local_count, capacity, group_count),
        out_shape=(
            jax.ShapeDtypeStruct((rows, query_weight.shape[1]), BF16),
            jax.ShapeDtypeStruct((rows, query_rotary.shape[1]), BF16),
            jax.ShapeDtypeStruct((tokens, group_count * local_count * capacity), BF16),
        ),
        in_specs=[SMEM_SPEC] + [VMEM_SPEC] * 7,
        out_specs=(VMEM_SPEC,) * 3,
        compiler_params=params(60),
        cost_estimate=cost(4e12 * 4e-6, 12e6),
        name="queries",
    )(
        ids, query_latent, gain.reshape(1, width), query_weight, query_rotary, cosine, sine,
        routes.T,
    )


def attention_kernel(
    turn_width, piece_count, tp_bits, ids, plain, turned, cosine, sine, key_weight,
    value_weight, output_hbm, *rest
):
    pieces = rest[:piece_count]
    keep, send, meta, keys, values, mixed, output_weight, sem = rest[piece_count:]
    fetch = pltpu.make_async_copy(output_hbm, output_weight, sem)
    fetch.start()
    rows = plain.shape[0]
    latent = key_weight.shape[0]
    turn_lanes = turned.shape[1]
    pair_count = keys.shape[0]
    pair = 2 * NOPE
    scale = LOG2E * (NOPE + turn_width) ** (-0.5)
    half = pieces[0].shape[0]
    repeat = turn_lanes // turn_width

    for index, piece in enumerate(pieces):
        name, side = index // 2, index % 2
        place = ids[1] if side == 0 else 1 - ids[1]
        base = pl.multiple_of(place * half, half)
        block = piece[:, :latent]
        start = index * half
        key_block = jnp.dot(block, key_weight[...], preferred_element_type=F32).astype(BF16)
        value_block = jnp.dot(block, value_weight[...], preferred_element_type=F32).astype(BF16)
        beside = piece[:, latent:].astype(F32)
        if name > 0:
            meta[name - 1, :, pl.ds(base, half)] = beside.T[turn_width : turn_width + 8, :]
        key = beside[:, :turn_width]
        key = jnp.concatenate([key] * repeat, axis=1)
        c, s = turn_tables(
            cosine, sine, pl.multiple_of(ids[3 + name] * rows + place * half, half), half,
            turn_lanes,
        )
        key = rotate_lanes(key, c, s, turn_width // 2).astype(BF16)
        for p in range(pair_count):
            keys[p, start : start + half, :pair] = key_block[:, p * pair : (p + 1) * pair]
            keys[p, start : start + half, pair:] = key
            values[p, start : start + half, :] = value_block[:, p * pair : (p + 1) * pair]

    tile = min(rows, 256)
    plain_lane = lax.broadcasted_iota(jnp.int32, (tile, pair), 1)
    turn_lane = lax.broadcasted_iota(jnp.int32, (tile, turn_lanes), 1)
    zero = jnp.zeros((), BF16)

    def step(index, carry):
        row = pl.ds(pl.multiple_of(index * tile, tile), tile)
        for p in range(pair_count):
            outs = []
            for h in range(2):
                head = 2 * p + h
                left = jnp.where(
                    (plain_lane // NOPE) == h, plain[row, p * pair : (p + 1) * pair], zero
                )
                right = jnp.where((turn_lane // turn_width) == head, turned[row, :], zero)
                query = jnp.concatenate([left, right], axis=1)
                scores = lax.dot_general(
                    query, keys[p], (((1,), (1,)), ((), ())), preferred_element_type=F32
                )
                top = jnp.max(scores, axis=1, keepdims=True)
                expo = jnp.exp2((scores - top) * scale)
                total = jnp.sum(expo, axis=1, keepdims=True)
                mix = jnp.dot(expo.astype(BF16), values[p], preferred_element_type=F32)
                outs.append(mix / total)
            mixed[row, p * pair : (p + 1) * pair] = jnp.where(
                plain_lane < VDIM, outs[0], outs[1]
            ).astype(BF16)
        return carry

    lax.fori_loop(0, rows // tile, step, 0)

    fetch.wait()
    place_count = 1 << tp_bits
    block_rows = rows // place_count
    me = ids[0]
    middle = place_count // 2
    for target, low in ((send, middle), (keep, 0)):
        parts = [
            mixed[
                pl.ds(
                    pl.multiple_of((me ^ spread(low + i, tp_bits)) * block_rows, block_rows),
                    block_rows,
                ),
                :,
            ]
            for i in range(middle)
        ]
        target[...] = jnp.dot(
            jnp.concatenate(parts, axis=0), output_weight[...], preferred_element_type=F32
        ).astype(BF16)


def attention(
    ids, plain, turned, cosine, sine, key_weight, value_weight, output_weight, pieces,
    turn_width, tp_bits,
):
    rows = plain.shape[0]
    head_count = key_weight.shape[1] // NOPE
    key_rows = sum(p.shape[0] for p in pieces)
    turn_lanes = turned.shape[1]
    width = output_weight.shape[1]
    shape = jax.ShapeDtypeStruct((rows // 2, width), BF16)
    return pl.pallas_call(
        functools.partial(attention_kernel, turn_width, len(pieces), tp_bits),
        out_shape=(shape, shape, jax.ShapeDtypeStruct((len(pieces) // 2 - 1, 8, rows), F32)),
        in_specs=[SMEM_SPEC] + [VMEM_SPEC] * 6 + [HBM_SPEC] + [VMEM_SPEC] * len(pieces),
        out_specs=(VMEM_SPEC,) * 3,
        scratch_shapes=[
            pltpu.VMEM((head_count // 2, key_rows, 2 * NOPE + turn_lanes), BF16),
            pltpu.VMEM((head_count // 2, key_rows, 2 * VDIM), BF16),
            pltpu.VMEM((rows, head_count * VDIM), BF16),
            pltpu.VMEM(output_weight.shape, BF16),
            pltpu.SemaphoreType.DMA,
        ],
        compiler_params=params(26 if key_rows <= 2048 else 60),
        cost_estimate=cost(4e12 * 12e-6, 40e6),
        name="attention",
    )(
        ids, plain, turned, cosine, sine, key_weight, value_weight, output_weight, *pieces
    )


def experts_kernel(
    names, group_count, capacity, tp_bits, ids, gate, up, down, own_meta, metas, *rest
):
    blocks = len(names)
    pieces = rest[: 2 * blocks]
    keep, send, slots, loads, gathered = rest[2 * blocks :]
    local_count = gate.shape[0]
    tokens = own_meta.shape[1]
    half = tokens // 2
    me, core, group = ids[0], ids[1], ids[2]

    before = (
        lax.broadcasted_iota(jnp.int32, (tokens, tokens), 0)
        < lax.broadcasted_iota(jnp.int32, (tokens, tokens), 1)
    ).astype(BF16)
    row = lax.broadcasted_iota(jnp.int32, (8, tokens), 0)
    wanted = (row + group * local_count).astype(F32)
    for b in range(blocks):
        meta = own_meta[...] if names[b] == 0 else metas[names[b] - 1]
        first = meta[0:1, :] == wanted
        second = meta[1:2, :] == wanted
        named = (first | second) & (row < local_count)
        rank = jnp.dot(named.astype(BF16), before, preferred_element_type=F32)
        slots[b] = jnp.where(named, rank, -1.0)
        loads[b] = jnp.where(first, meta[2:3, :] + meta[4:5, :] + meta[6:7, :], 0.0) + jnp.where(
            second, meta[3:4, :] + meta[5:6, :] + meta[7:8, :], 0.0
        )

    own = pl.multiple_of(core * half, half)
    far = pl.multiple_of((1 - core) * half, half)
    place = lax.broadcasted_iota(jnp.int32, (capacity, half), 0).astype(F32)
    place_count = 1 << tp_bits
    part = down.shape[2] // place_count
    for j in range(local_count):
        scale = []
        for b in range(blocks):
            hits, weight = [], None
            for offset in (own, far):
                hit = place == slots[b, j : j + 1, pl.ds(offset, half)]
                load = jnp.where(hit, loads[b, j : j + 1, pl.ds(offset, half)], 0.0)
                load = jnp.sum(load, axis=1, keepdims=True)
                weight = load if weight is None else weight + load
                hits.append(jnp.where(hit, 1.0, 0.0).astype(BF16))
            block = jnp.concatenate([pieces[2 * b][...], pieces[2 * b + 1][...]], axis=0)
            gathered[b * capacity : (b + 1) * capacity, :] = jnp.dot(
                jnp.concatenate(hits, axis=1), block, preferred_element_type=F32
            ).astype(BF16)
            scale.append(weight)
        rows_in = gathered[...]
        gate_acts = jnp.dot(rows_in, gate[j], preferred_element_type=F32)
        up_acts = jnp.dot(rows_in, up[j], preferred_element_type=F32)
        hidden = (gate_acts * (1.0 / (1.0 + jnp.exp(-gate_acts))) * up_acts).astype(BF16)
        for target, low in ((send, place_count // 2), (keep, 0)):
            for i in range(place_count // 2):
                column = pl.multiple_of((me ^ spread(low + i, tp_bits)) * part, part)
                product = jnp.dot(
                    hidden, down[j, :, pl.ds(column, part)], preferred_element_type=F32
                )
                for b in range(blocks):
                    base = pl.multiple_of(
                        (ids[3 + group_count + names[b]] * local_count + j) * capacity, capacity
                    )
                    target[pl.ds(base, capacity), i * part : (i + 1) * part] = (
                        product[b * capacity : (b + 1) * capacity, :] * scale[b]
                    ).astype(BF16)


def run_experts(
    ids, names, own_meta, metas, pieces, gate_weight, up_weight, down_weight, capacity, tp_bits
):
    local_count, width, _ = gate_weight.shape
    count = len(names)
    tokens = own_meta.shape[1]
    rows = count * local_count * capacity
    shape = jax.ShapeDtypeStruct((rows, width // 2), BF16)
    return pl.pallas_call(
        functools.partial(
            experts_kernel, tuple(names), metas.shape[0] + 1, capacity, tp_bits
        ),
        out_shape=(shape, shape),
        in_specs=[SMEM_SPEC] + [VMEM_SPEC] * (5 + 2 * count),
        out_specs=(VMEM_SPEC, VMEM_SPEC),
        scratch_shapes=[
            pltpu.VMEM((count, 8, tokens), F32),
            pltpu.VMEM((count, 8, tokens), F32),
            pltpu.VMEM((count * capacity, width), BF16),
        ],
        compiler_params=params(min(60, 18 + 4 * count)),
        cost_estimate=cost(4e12 * 5e-6 * count, 14e6 * count),
        name="experts",
    )(ids, gate_weight, up_weight, down_weight, own_meta, metas, *pieces)


def combine_kernel(starts, pick, *rest):
    out = rest[-1]
    count = len(starts)
    total = None
    for start, part in zip(starts, rest[:count]):
        span = part.shape[0]
        found = jnp.dot(pick[:, start : start + span], part[...], preferred_element_type=F32)
        total = found if total is None else total + found
    for carry in rest[count:-1]:
        total = total + carry[...].astype(F32)
    out[...] = total.astype(BF16)


def combine(pick, parts, carries):
    tokens = pick.shape[0]
    names = sorted(parts)
    span, width = parts[names[0]].shape
    operands = [parts[r] for r in names] + list(carries)
    return pl.pallas_call(
        functools.partial(combine_kernel, tuple(r * span for r in names)),
        out_shape=jax.ShapeDtypeStruct((tokens, width), BF16),
        in_specs=[VMEM_SPEC] * (1 + len(operands)),
        out_specs=VMEM_SPEC,
        compiler_params=params(24),
        cost_estimate=cost(4e12 * 1e-6, 4e6),
        name="combine",
    )(pick, *operands)


def low_bit(value):
    return value & -value


def reverse_bits(value, bits):
    return sum(((value >> b) & 1) << (bits - 1 - b) for b in range(bits))


def step_over(value, bit, ep_bits):
    groups, parts = lax.axis_size("ep"), lax.axis_size("tp")
    pairs = []
    for e in range(groups):
        for t in range(parts):
            mask = 1 << (bit if t % 2 == 0 else ep_bits - 1 - bit)
            pairs.append((e * parts + t, (e ^ mask) * parts + t))
    return lax.ppermute(value, ("ep", "tp"), pairs)


def add_wide(left, right):
    return (left.astype(F32) + right.astype(F32)).astype(BF16)


def local(
    query_latent,
    joint_latent,
    rotary_key,
    query_gain,
    joint_gain,
    query_weight,
    query_rotary,
    key_weight,
    value_weight,
    output_weight,
    expert_input,
    expert_gain,
    routes,
    route_weight,
    gate_weight,
    up_weight,
    down_weight,
):
    group_count = lax.axis_size("ep")
    part_count = lax.axis_size("tp")
    ep_bits, tp_bits = bits_of(group_count), bits_of(part_count)
    ep, tp = lax.axis_index("ep"), lax.axis_index("tp")
    core = tp & 1
    names = range(group_count)
    groups = [ep ^ jnp.where(core == 0, n, reverse_bits(n, ep_bits)) for n in names]
    near = [n for n in names if bin(n).count("1") <= 1]
    far = [n for n in names if n not in near]
    classes = [near] + ([far] if far else [])
    place = {n: c.index(n) for c in classes for n in c}
    orders = [jnp.where(core == 0, place[n], place[reverse_bits(n, ep_bits)]) for n in names]
    ids = jnp.stack([tp, core, ep] + groups + orders).astype(jnp.int32)
    rows = query_latent.shape[0]
    turn_width = rotary_key.shape[1]
    local_count = gate_weight.shape[0]
    tokens = expert_input.shape[0]
    capacity = 3 * tokens // (2 * group_count)
    half_width = turn_width // 2

    latent_mine, latent_other, own_meta, row_mine, row_other = prepare(
        ids, joint_latent, joint_gain, rotary_key, routes, route_weight, expert_input,
        expert_gain,
    )
    latent_held = {0: latent_mine}
    for b in range(ep_bits):
        latent_held[1 << b] = step_over(latent_mine, b, ep_bits)
    row_held = {0: row_mine, 1: step_over(row_mine, 0, ep_bits)}

    positions = jnp.arange(rows * group_count, dtype=jnp.int32).astype(F32)
    frequencies = ROTARY_BASE ** (-jnp.arange(half_width, dtype=F32) / half_width)
    angles = frequencies[:, None] * positions[None, :]
    cosine, sine = jnp.cos(angles), jnp.sin(angles)
    plain, turned, pick = queries(
        ids, query_latent, query_gain, query_weight, query_rotary, cosine,
        sine, routes, turn_width, local_count, capacity, group_count,
    )
    for n in far:
        b = n.bit_length() - 1
        latent_held[n] = step_over(latent_held[n ^ (1 << b)], b, ep_bits)
    for b in range(1, ep_bits):
        row_held[1 << b] = step_over(row_mine, b, ep_bits)

    def with_other(values, own_other):
        swapped = {n: swap_over(values[n], "tp", 1) for n in names if n}
        return {
            n: [values[n], swapped[reverse_bits(n, ep_bits)] if n else own_other] for n in names
        }

    latents = with_other(latent_held, latent_other)
    keep, send, metas = attention(
        ids, plain, turned, cosine, sine, key_weight, value_weight, output_weight,
        [piece for n in names for piece in latents[n]], turn_width, tp_bits,
    )
    for n in far:
        b = n.bit_length() - 1
        row_held[n] = step_over(row_held[n ^ (1 << b)], b, ep_bits)
    arrived = swap_over(send, "tp", 1)
    for b in range(1, tp_bits):
        cut = keep.shape[0] // 2
        away = add_wide(keep[cut:], arrived[cut:])
        keep = add_wide(keep[:cut], arrived[:cut])
        arrived = swap_over(away, "tp", 1 << b)
    mixer_out = add_wide(keep, arrived)

    row_pairs = with_other(row_held, row_other)
    parts = {}
    span = local_count * capacity
    chunk_count = part_count // 2
    width = expert_input.shape[1] // part_count
    gathered = {}
    for chosen in classes:
        keep, send = run_experts(
            ids, chosen, own_meta, metas, [piece for n in chosen for piece in row_pairs[n]],
            gate_weight, up_weight, down_weight, capacity, tp_bits,
        )
        arrived = swap_over(send, "tp", 1)
        if chosen == near:
            both = add_wide(keep, arrived)
            for i, r in enumerate(chosen):
                for c in range(chunk_count):
                    parts[r, c] = both[i * span : (i + 1) * span, c * width : (c + 1) * width]
        else:
            for b in range(1, tp_bits):
                cut = keep.shape[1] // 2
                away = add_wide(keep[:, cut:], arrived[:, cut:])
                keep = add_wide(keep[:, :cut], arrived[:, :cut])
                arrived = swap_over(away, "tp", 1 << b)
            both = add_wide(keep, arrived)
            for i, r in enumerate(chosen):
                gathered[r] = swap_over(both[i * span : (i + 1) * span], "ep", r)

    carried = {}
    for c in sorted(range(chunk_count), key=lambda i: -spread(i, tp_bits)):
        mask = spread(c, tp_bits)
        found = {r: swap_over(parts[r, c], "ep", r) if r else parts[r, c] for r in near}
        if not mask:
            found.update(gathered)
        total = combine(pick, found, carried.pop(mask, []))
        if mask:
            arrived = swap_over(total, "tp", low_bit(mask))
            carried.setdefault(mask ^ low_bit(mask), []).append(arrived)
    expert_out = total
    return (mixer_out, expert_out)


def solution(mesh):
    return jax.shard_map(
        local,
        mesh=mesh,
        in_specs=(
            P("ep", None),
            P("ep", None),
            P("ep", None),
            P(),
            P(),
            P(None, "tp"),
            P(None, "tp"),
            P(None, "tp"),
            P(None, "tp"),
            P("tp", None),
            P("ep", None),
            P(),
            P("ep", None),
            P("ep", None),
            P("ep", None, "tp"),
            P("ep", None, "tp"),
            P("ep", "tp", None),
        ),
        out_specs=(P(("ep", "tp"), None), P("ep", "tp")),
        check_vma=False,
    )
```

```python
import functools

import jax
import jax.numpy as jnp
from jax import lax
from jax.experimental import pallas as pl
from jax.experimental.pallas import tpu as pltpu
from jax.sharding import PartitionSpec as P


NOPE = 64
VDIM = 64
NORM_EPSILON = 1e-06
ROTARY_BASE = 10000.0
LOG2E = 1.4426950408889634

F32 = jnp.float32
BF16 = jnp.bfloat16

SMEM_SPEC = pl.BlockSpec(memory_space=pltpu.SMEM)
VMEM_SPEC = pl.BlockSpec(memory_space=pltpu.VMEM)
HBM_SPEC = pl.BlockSpec(memory_space=pltpu.HBM)


def in_hbm(value):
    return pltpu.with_memory_space_constraint(value, pltpu.HBM)


def params(mebibytes):
    return pltpu.CompilerParams(vmem_limit_bytes=mebibytes * 1024 * 1024)


def cost(flops, bytes_accessed):
    return pl.CostEstimate(
        flops=int(flops), bytes_accessed=int(bytes_accessed), transcendentals=0
    )


def swap_over(value, axis, mask):
    size = lax.axis_size(axis)
    return lax.ppermute(value, axis, [(i, i ^ mask) for i in range(size)])


def bits_of(size):
    return max(size - 1, 0).bit_length()


def spread(index, bits):
    return sum(((index >> (bits - 1 - b)) & 1) << b for b in range(bits))


def norm_value(source, gain):
    wide = source.astype(F32)
    factor = lax.rsqrt(jnp.mean(wide * wide, axis=-1, keepdims=True) + NORM_EPSILON)
    return (wide * factor * gain).astype(BF16)


def rotate_lanes(source, cosine, sine, half):
    width = source.shape[-1]
    lane = lax.broadcasted_iota(jnp.int32, source.shape, 1)
    first = (lane & (2 * half - 1)) < half
    partner = jnp.where(
        first, pltpu.roll(source, width - half, 1), pltpu.roll(source, half, 1)
    )
    return source * cosine + partner * sine


def prepare_kernel(
    ids, joint_hbm, joint_gain_hbm, rotary_hbm, routes_hbm, weights_hbm, rows_hbm, rows_gain_hbm,
    mine_hbm, other_hbm, meta_hbm, row_mine_hbm, row_other_hbm,
    joint, joint_gain, rotary, routes, weights, rows, rows_gain,
    mine, other, meta, row_mine, row_other, sems,
):
    inputs = (
        (joint_hbm, joint), (joint_gain_hbm, joint_gain), (rotary_hbm, rotary),
        (routes_hbm, routes), (weights_hbm, weights), (rows_gain_hbm, rows_gain), (rows_hbm, rows),
    )
    loads = [
        pltpu.make_async_copy(source, target, sems.at[i])
        for i, (source, target) in enumerate(inputs)
    ]
    outputs = (
        (mine, mine_hbm), (other, other_hbm), (meta, meta_hbm), (row_mine, row_mine_hbm),
        (row_other, row_other_hbm),
    )
    stores = [
        pltpu.make_async_copy(source, target, sems.at[len(loads) + i])
        for i, (source, target) in enumerate(outputs)
    ]
    for load in loads:
        load.start()
    for load in loads[:5]:
        load.wait()
    half, full = mine.shape
    count, width = joint.shape
    turn, top = rotary.shape[0], routes.shape[0]
    weight = weights[...]
    high = weight.astype(BF16).astype(F32)
    middle = (weight - high).astype(BF16).astype(F32)
    low = weight - high - middle
    rest = jnp.zeros((full - width - turn - 4 * top, count), F32)
    named = routes[...].astype(F32)
    meta[...] = jnp.concatenate([named, weight, rest[: 8 - 2 * top]], axis=0)
    side = jnp.concatenate(
        [rotary[...].astype(F32), named, high, middle, low, rest], axis=0
    ).T.astype(BF16)
    chosen = ids[1] == 0
    mine[:, width:] = jnp.where(chosen, side[:half], side[half:])
    other[:, width:] = jnp.where(chosen, side[half:], side[:half])
    own = pl.multiple_of(ids[1] * half, half)
    far = pl.multiple_of((1 - ids[1]) * half, half)
    mine[:, :width] = norm_value(joint[pl.ds(own, half), :], joint_gain[...])
    stores[0].start()
    other[:, :width] = norm_value(joint[pl.ds(far, half), :], joint_gain[...])
    stores[1].start()
    stores[2].start()
    for load in loads[5:]:
        load.wait()
    row_mine[...] = norm_value(rows[pl.ds(own, half), :], rows_gain[...])
    stores[3].start()
    row_other[...] = norm_value(rows[pl.ds(far, half), :], rows_gain[...])
    stores[4].start()
    for store in stores:
        store.wait()


def prepare(ids, joint, joint_gain, rotary, routes, weights, rows, rows_gain):
    count, width = joint.shape
    half = count // 2
    inputs = (
        joint, joint_gain.reshape(1, width), rotary.T, routes.T, weights.T, rows,
        rows_gain.reshape(1, rows.shape[1]),
    )
    outputs = (
        jax.ShapeDtypeStruct((half, width + 128), BF16),
        jax.ShapeDtypeStruct((half, width + 128), BF16),
        jax.ShapeDtypeStruct((8, count), F32),
        jax.ShapeDtypeStruct((half, rows.shape[1]), BF16),
        jax.ShapeDtypeStruct((half, rows.shape[1]), BF16),
    )
    return pl.pallas_call(
        prepare_kernel,
        out_shape=outputs,
        in_specs=[SMEM_SPEC] + [HBM_SPEC] * len(inputs),
        out_specs=(HBM_SPEC,) * len(outputs),
        scratch_shapes=[pltpu.VMEM(v.shape, v.dtype) for v in inputs + outputs]
        + [pltpu.SemaphoreType.DMA((len(inputs) + len(outputs),))],
        compiler_params=params(60),
        cost_estimate=cost(4e12 * 3e-6, 4e6),
        name="prepare",
    )(ids, *[in_hbm(v) for v in inputs])


def turn_tables(cosine, sine, start, count, lanes):
    turned = pl.ds(start, count)
    half = cosine.shape[0]
    repeat = lanes // (2 * half)
    c, s = cosine[:, turned], sine[:, turned]
    return (
        jnp.concatenate([c, c] * repeat, axis=0).T,
        jnp.concatenate([-s, s] * repeat, axis=0).T,
    )


def pick_value(local_count, capacity, group_count, ids, routes, out):
    tokens = routes.shape[1]
    group = ids[2]
    total = group_count * local_count
    row = lax.broadcasted_iota(jnp.int32, (total, tokens), 0)
    expert = ((group ^ (row // local_count)) * local_count + row % local_count)
    first = routes[0:1, :] == expert
    second = routes[1:2, :] == expert
    before = (
        lax.broadcasted_iota(jnp.int32, (tokens, tokens), 0)
        < lax.broadcasted_iota(jnp.int32, (tokens, tokens), 1)
    ).astype(BF16)
    named = jnp.where(first | second, 1.0, 0.0).astype(BF16)
    slot = jnp.dot(named, before, preferred_element_type=F32) + (row * capacity).astype(F32)
    pair = jnp.concatenate(
        [
            jnp.sum(jnp.where(first, slot, 0.0), axis=0, keepdims=True),
            jnp.sum(jnp.where(second, slot, 0.0), axis=0, keepdims=True),
            jnp.zeros((126, tokens), F32),
        ],
        axis=0,
    ).T
    span = 128
    for start in range(0, total * capacity, span):
        place = (lax.broadcasted_iota(jnp.int32, (tokens, span), 1) + start).astype(F32)
        out[:, start : start + span] = jnp.where(
            (place == pair[:, 0:1]) | (place == pair[:, 1:2]), 1.0, 0.0
        ).astype(BF16)


def query_kernel(
    turn_width, local_count, capacity, group_count, ids, query_latent, gain, query_weight,
    query_rotary, cosine, sine, routes, plain, turned, pick
):
    rows = query_latent.shape[0]
    normed = norm_value(query_latent[...], gain[...])
    plain[...] = jnp.dot(normed, query_weight[...], preferred_element_type=F32).astype(BF16)
    start = pl.multiple_of(ids[2] * rows, rows)
    c, s = turn_tables(cosine, sine, start, rows, turned.shape[1])
    turned[...] = rotate_lanes(
        jnp.dot(normed, query_rotary[...], preferred_element_type=F32), c, s, turn_width // 2
    ).astype(BF16)
    pick_value(local_count, capacity, group_count, ids, routes, pick)


def queries(
    ids, query_latent, gain, query_weight, query_rotary, cosine, sine, routes, turn_width,
    local_count, capacity, group_count,
):
    rows, width = query_latent.shape
    tokens = routes.shape[0]
    return pl.pallas_call(
        functools.partial(query_kernel, turn_width, local_count, capacity, group_count),
        out_shape=(
            jax.ShapeDtypeStruct((rows, query_weight.shape[1]), BF16),
            jax.ShapeDtypeStruct((rows, query_rotary.shape[1]), BF16),
            jax.ShapeDtypeStruct((tokens, group_count * local_count * capacity), BF16),
        ),
        in_specs=[SMEM_SPEC] + [VMEM_SPEC] * 7,
        out_specs=(VMEM_SPEC,) * 3,
        compiler_params=params(60),
        cost_estimate=cost(4e12 * 4e-6, 12e6),
        name="queries",
    )(
        ids, query_latent, gain.reshape(1, width), query_weight, query_rotary, cosine, sine,
        routes.T,
    )


def attention_kernel(
    turn_width, piece_count, tp_bits, ids, *rest
):
    sources = rest[:7]
    pieces = rest[7 : 7 + piece_count]
    keep, send, meta, keys, values, mixed = rest[7 + piece_count : 13 + piece_count]
    targets = rest[13 + piece_count : 20 + piece_count]
    sems = rest[-1]
    key_weight, value_weight, cosine, sine, plain, turned, output_weight = targets
    loads = [
        pltpu.make_async_copy(source, target, sems.at[i])
        for i, (source, target) in enumerate(zip(sources, targets))
    ]
    for load in loads:
        load.start()
    for load in loads[:4]:
        load.wait()
    rows = plain.shape[0]
    latent = key_weight.shape[0]
    turn_lanes = turned.shape[1]
    pair_count = keys.shape[0]
    pair = 2 * NOPE
    scale = LOG2E * (NOPE + turn_width) ** (-0.5)
    half = pieces[0].shape[0]
    repeat = turn_lanes // turn_width

    for index, piece in enumerate(pieces):
        name, side = index // 2, index % 2
        place = ids[1] if side == 0 else 1 - ids[1]
        base = pl.multiple_of(place * half, half)
        block = piece[:, :latent]
        start = index * half
        key_block = jnp.dot(block, key_weight[...], preferred_element_type=F32).astype(BF16)
        value_block = jnp.dot(block, value_weight[...], preferred_element_type=F32).astype(BF16)
        beside = piece[:, latent:].astype(F32)
        if name > 0:
            meta[name - 1, :, pl.ds(base, half)] = beside.T[turn_width : turn_width + 8, :]
        key = beside[:, :turn_width]
        key = jnp.concatenate([key] * repeat, axis=1)
        c, s = turn_tables(
            cosine, sine, pl.multiple_of(ids[3 + name] * rows + place * half, half), half,
            turn_lanes,
        )
        key = rotate_lanes(key, c, s, turn_width // 2).astype(BF16)
        for p in range(pair_count):
            keys[p, start : start + half, :pair] = key_block[:, p * pair : (p + 1) * pair]
            keys[p, start : start + half, pair:] = key
            values[p, start : start + half, :] = value_block[:, p * pair : (p + 1) * pair]

    loads[4].wait()
    loads[5].wait()
    tile = min(rows, 256)
    plain_lane = lax.broadcasted_iota(jnp.int32, (tile, pair), 1)
    turn_lane = lax.broadcasted_iota(jnp.int32, (tile, turn_lanes), 1)
    zero = jnp.zeros((), BF16)

    def step(index, carry):
        row = pl.ds(pl.multiple_of(index * tile, tile), tile)
        for p in range(pair_count):
            outs = []
            for h in range(2):
                head = 2 * p + h
                left = jnp.where(
                    (plain_lane // NOPE) == h, plain[row, p * pair : (p + 1) * pair], zero
                )
                right = jnp.where((turn_lane // turn_width) == head, turned[row, :], zero)
                query = jnp.concatenate([left, right], axis=1)
                scores = lax.dot_general(
                    query, keys[p], (((1,), (1,)), ((), ())), preferred_element_type=F32
                )
                top = jnp.max(scores, axis=1, keepdims=True)
                expo = jnp.exp2((scores - top) * scale)
                total = jnp.sum(expo, axis=1, keepdims=True)
                mix = jnp.dot(expo.astype(BF16), values[p], preferred_element_type=F32)
                outs.append(mix / total)
            mixed[row, p * pair : (p + 1) * pair] = jnp.where(
                plain_lane < VDIM, outs[0], outs[1]
            ).astype(BF16)
        return carry

    lax.fori_loop(0, rows // tile, step, 0)

    loads[6].wait()
    place_count = 1 << tp_bits
    block_rows = rows // place_count
    me = ids[0]
    middle = place_count // 2
    for target, low in ((send, middle), (keep, 0)):
        parts = [
            mixed[
                pl.ds(
                    pl.multiple_of((me ^ spread(low + i, tp_bits)) * block_rows, block_rows),
                    block_rows,
                ),
                :,
            ]
            for i in range(middle)
        ]
        target[...] = jnp.dot(
            jnp.concatenate(parts, axis=0), output_weight[...], preferred_element_type=F32
        ).astype(BF16)


def attention(
    ids, plain, turned, cosine, sine, key_weight, value_weight, output_weight, pieces,
    turn_width, tp_bits,
):
    rows = plain.shape[0]
    head_count = key_weight.shape[1] // NOPE
    key_rows = sum(p.shape[0] for p in pieces)
    sources = (key_weight, value_weight, cosine, sine, plain, turned, output_weight)
    turn_lanes = turned.shape[1]
    width = output_weight.shape[1]
    shape = jax.ShapeDtypeStruct((rows // 2, width), BF16)
    return pl.pallas_call(
        functools.partial(attention_kernel, turn_width, len(pieces), tp_bits),
        out_shape=(shape, shape, jax.ShapeDtypeStruct((len(pieces) // 2 - 1, 8, rows), F32)),
        in_specs=[SMEM_SPEC] + [HBM_SPEC] * 7 + [VMEM_SPEC] * len(pieces),
        out_specs=(VMEM_SPEC,) * 3,
        scratch_shapes=[
            pltpu.VMEM((head_count // 2, key_rows, 2 * NOPE + turn_lanes), BF16),
            pltpu.VMEM((head_count // 2, key_rows, 2 * VDIM), BF16),
            pltpu.VMEM((rows, head_count * VDIM), BF16),
        ]
        + [pltpu.VMEM(v.shape, v.dtype) for v in sources]
        + [
            pltpu.SemaphoreType.DMA((7,)),
        ],
        compiler_params=params(26 if key_rows <= 2048 else 60),
        cost_estimate=cost(4e12 * 12e-6, 40e6),
        name="attention",
    )(ids, *[in_hbm(v) for v in sources], *pieces)


def experts_kernel(
    names, fetch, group_count, capacity, tp_bits, ids, gate, up, down, *rest
):
    blocks = len(names)
    tables = rest[:blocks]
    pieces = rest[blocks : 3 * blocks]
    if fetch:
        sources = (gate, up, down)
        keep, send, gate, up, down, slots, loads, gathered, sems = rest[3 * blocks :]
        copies = [
            pltpu.make_async_copy(source.at[j], target.at[j], sems.at[3 * j + k])
            for j in range(gate.shape[0])
            for k, (source, target) in enumerate(zip(sources, (gate, up, down)))
        ]
        for copy in copies:
            copy.start()
    else:
        keep, send, slots, loads, gathered = rest[3 * blocks :]
    local_count = gate.shape[0]
    tokens = tables[0].shape[1]
    half = tokens // 2
    me, core, group = ids[0], ids[1], ids[2]

    before = (
        lax.broadcasted_iota(jnp.int32, (tokens, tokens), 0)
        < lax.broadcasted_iota(jnp.int32, (tokens, tokens), 1)
    ).astype(BF16)
    row = lax.broadcasted_iota(jnp.int32, (8, tokens), 0)
    wanted = (row + group * local_count).astype(F32)
    for b in range(blocks):
        meta = tables[b][...]
        first = meta[0:1, :] == wanted
        second = meta[1:2, :] == wanted
        named = (first | second) & (row < local_count)
        rank = jnp.dot(named.astype(BF16), before, preferred_element_type=F32)
        slots[b] = jnp.where(named, rank, -1.0)
        loads[b] = jnp.where(first, meta[2:3, :] + meta[4:5, :] + meta[6:7, :], 0.0) + jnp.where(
            second, meta[3:4, :] + meta[5:6, :] + meta[7:8, :], 0.0
        )

    own = pl.multiple_of(core * half, half)
    far = pl.multiple_of((1 - core) * half, half)
    place = lax.broadcasted_iota(jnp.int32, (capacity, half), 0).astype(F32)
    place_count = 1 << tp_bits
    part = down.shape[2] // place_count
    for j in range(local_count):
        scale = []
        for b in range(blocks):
            hits, weight = [], None
            for offset in (own, far):
                hit = place == slots[b, j : j + 1, pl.ds(offset, half)]
                load = jnp.where(hit, loads[b, j : j + 1, pl.ds(offset, half)], 0.0)
                load = jnp.sum(load, axis=1, keepdims=True)
                weight = load if weight is None else weight + load
                hits.append(jnp.where(hit, 1.0, 0.0).astype(BF16))
            block = jnp.concatenate([pieces[2 * b][...], pieces[2 * b + 1][...]], axis=0)
            gathered[b * capacity : (b + 1) * capacity, :] = jnp.dot(
                jnp.concatenate(hits, axis=1), block, preferred_element_type=F32
            ).astype(BF16)
            scale.append(weight)
        rows_in = gathered[...]
        if fetch:
            copies[3 * j].wait()
        gate_acts = jnp.dot(rows_in, gate[j], preferred_element_type=F32)
        if fetch:
            copies[3 * j + 1].wait()
        up_acts = jnp.dot(rows_in, up[j], preferred_element_type=F32)
        if fetch:
            copies[3 * j + 2].wait()
        hidden = (gate_acts * (1.0 / (1.0 + jnp.exp(-gate_acts))) * up_acts).astype(BF16)
        for target, low in ((send, place_count // 2), (keep, 0)):
            for i in range(place_count // 2):
                column = pl.multiple_of((me ^ spread(low + i, tp_bits)) * part, part)
                product = jnp.dot(
                    hidden, down[j, :, pl.ds(column, part)], preferred_element_type=F32
                )
                for b in range(blocks):
                    base = pl.multiple_of(
                        (ids[3 + group_count + names[b]] * local_count + j) * capacity, capacity
                    )
                    target[pl.ds(base, capacity), i * part : (i + 1) * part] = (
                        product[b * capacity : (b + 1) * capacity, :] * scale[b]
                    ).astype(BF16)


def run_experts(ids, group_count, names, tables, pieces, weights, fetch, capacity, tp_bits):
    local_count, width, _ = weights[0].shape
    count = len(names)
    tokens = tables[0].shape[1]
    rows = count * local_count * capacity
    shapes = [jax.ShapeDtypeStruct((rows, width // 2), BF16)] * 2
    scratch = [
        pltpu.VMEM((count, 8, tokens), F32),
        pltpu.VMEM((count, 8, tokens), F32),
        pltpu.VMEM((count * capacity, width), BF16),
    ]
    if fetch:
        shapes += [pltpu.VMEM(w.shape, w.dtype) for w in weights]
        scratch.append(pltpu.SemaphoreType.DMA((3 * local_count,)))
    return pl.pallas_call(
        functools.partial(
            experts_kernel, tuple(names), fetch, group_count, capacity, tp_bits
        ),
        out_shape=tuple(shapes),
        in_specs=[SMEM_SPEC]
        + [HBM_SPEC if fetch else VMEM_SPEC] * 3
        + [VMEM_SPEC] * (3 * count),
        out_specs=(VMEM_SPEC,) * len(shapes),
        scratch_shapes=scratch,
        compiler_params=params(24 if fetch else min(60, 18 + 4 * count)),
        cost_estimate=cost(4e12 * 5e-6 * count, 14e6 * count),
        name="experts",
    )(ids, *([in_hbm(w) for w in weights] if fetch else weights), *tables, *pieces)


def combine_kernel(starts, pick, *rest):
    out = rest[-1]
    count = len(starts)
    total = None
    for start, part in zip(starts, rest[:count]):
        span = part.shape[0]
        found = jnp.dot(pick[:, start : start + span], part[...], preferred_element_type=F32)
        total = found if total is None else total + found
    for carry in rest[count:-1]:
        total = total + carry[...].astype(F32)
    out[...] = total.astype(BF16)


def combine(pick, parts, carries):
    tokens = pick.shape[0]
    names = sorted(parts)
    span, width = parts[names[0]].shape
    operands = [parts[r] for r in names] + list(carries)
    return pl.pallas_call(
        functools.partial(combine_kernel, tuple(r * span for r in names)),
        out_shape=jax.ShapeDtypeStruct((tokens, width), BF16),
        in_specs=[VMEM_SPEC] * (1 + len(operands)),
        out_specs=VMEM_SPEC,
        compiler_params=params(24),
        cost_estimate=cost(4e12 * 1e-6, 4e6),
        name="combine",
    )(pick, *operands)


def low_bit(value):
    return value & -value


def reverse_bits(value, bits):
    return sum(((value >> b) & 1) << (bits - 1 - b) for b in range(bits))


def step_over(value, bit, ep_bits):
    groups, parts = lax.axis_size("ep"), lax.axis_size("tp")
    pairs = []
    for e in range(groups):
        for t in range(parts):
            mask = 1 << (bit if t % 2 == 0 else ep_bits - 1 - bit)
            pairs.append((e * parts + t, (e ^ mask) * parts + t))
    return lax.ppermute(value, ("ep", "tp"), pairs)


def add_wide(left, right):
    return (left.astype(F32) + right.astype(F32)).astype(BF16)


def local(
    query_latent,
    joint_latent,
    rotary_key,
    query_gain,
    joint_gain,
    query_weight,
    query_rotary,
    key_weight,
    value_weight,
    output_weight,
    expert_input,
    expert_gain,
    routes,
    route_weight,
    gate_weight,
    up_weight,
    down_weight,
):
    group_count = lax.axis_size("ep")
    part_count = lax.axis_size("tp")
    ep_bits, tp_bits = bits_of(group_count), bits_of(part_count)
    ep, tp = lax.axis_index("ep"), lax.axis_index("tp")
    core = tp & 1
    names = range(group_count)
    groups = [ep ^ jnp.where(core == 0, n, reverse_bits(n, ep_bits)) for n in names]
    direct = [n for n in names if bin(n).count("1") == 1]
    far = [n for n in names if bin(n).count("1") > 1]
    near = [0] + direct
    classes = [[0], direct] + ([far] if far else [])
    place = {n: c.index(n) for c in classes for n in c}
    orders = [jnp.where(core == 0, place[n], place[reverse_bits(n, ep_bits)]) for n in names]
    ids = jnp.stack([tp, core, ep] + groups + orders).astype(jnp.int32)
    rows = query_latent.shape[0]
    turn_width = rotary_key.shape[1]
    local_count = gate_weight.shape[0]
    tokens = expert_input.shape[0]
    capacity = 3 * tokens // (2 * group_count)
    half_width = turn_width // 2

    latent_mine, latent_other, own_meta, row_mine, row_other = prepare(
        ids, joint_latent, joint_gain, rotary_key, routes, route_weight, expert_input,
        expert_gain,
    )
    latent_held = {0: latent_mine}
    for b in range(ep_bits):
        latent_held[1 << b] = step_over(latent_mine, b, ep_bits)
    row_held = {0: row_mine, 1: step_over(row_mine, 0, ep_bits)}

    positions = jnp.arange(rows * group_count, dtype=jnp.int32).astype(F32)
    frequencies = ROTARY_BASE ** (-jnp.arange(half_width, dtype=F32) / half_width)
    angles = frequencies[:, None] * positions[None, :]
    cosine, sine = jnp.cos(angles), jnp.sin(angles)
    plain, turned, pick = queries(
        ids, query_latent, query_gain, query_weight, query_rotary, cosine,
        sine, routes, turn_width, local_count, capacity, group_count,
    )
    for n in far:
        b = n.bit_length() - 1
        latent_held[n] = step_over(latent_held[n ^ (1 << b)], b, ep_bits)
    own_keep, own_send, *weights = run_experts(
        ids, group_count, [0], [own_meta], [row_mine, row_other],
        (gate_weight, up_weight, down_weight), True, capacity, tp_bits,
    )

    for b in range(1, ep_bits):
        row_held[1 << b] = step_over(row_mine, b, ep_bits)

    def with_other(values, own_other):
        swapped = {n: swap_over(values[n], "tp", 1) for n in names if n}
        return {
            n: [values[n], swapped[reverse_bits(n, ep_bits)] if n else own_other] for n in names
        }

    latents = with_other(latent_held, latent_other)
    keep, send, metas = attention(
        ids, plain, turned, cosine, sine, key_weight, value_weight, output_weight,
        [piece for n in names for piece in latents[n]], turn_width, tp_bits,
    )
    for n in far:
        b = n.bit_length() - 1
        row_held[n] = step_over(row_held[n ^ (1 << b)], b, ep_bits)
    arrived = swap_over(send, "tp", 1)
    for b in range(1, tp_bits):
        cut = keep.shape[0] // 2
        away = add_wide(keep[cut:], arrived[cut:])
        keep = add_wide(keep[:cut], arrived[:cut])
        arrived = swap_over(away, "tp", 1 << b)
    mixer_out = add_wide(keep, arrived)

    row_pairs = with_other(row_held, row_other)
    parts = {}
    span = local_count * capacity
    chunk_count = part_count // 2
    width = expert_input.shape[1] // part_count
    gathered = {}
    for chosen in classes:
        if chosen == [0]:
            keep, send = own_keep, own_send
        else:
            keep, send = run_experts(
                ids, group_count, chosen, [metas[n - 1] for n in chosen],
                [piece for n in chosen for piece in row_pairs[n]], weights, False,
                capacity, tp_bits,
            )
        arrived = swap_over(send, "tp", 1)
        if chosen != far:
            both = add_wide(keep, arrived)
            for i, r in enumerate(chosen):
                for c in range(chunk_count):
                    parts[r, c] = both[i * span : (i + 1) * span, c * width : (c + 1) * width]
        else:
            for b in range(1, tp_bits):
                cut = keep.shape[1] // 2
                away = add_wide(keep[:, cut:], arrived[:, cut:])
                keep = add_wide(keep[:, :cut], arrived[:, :cut])
                arrived = swap_over(away, "tp", 1 << b)
            both = add_wide(keep, arrived)
            for i, r in enumerate(chosen):
                gathered[r] = swap_over(both[i * span : (i + 1) * span], "ep", r)

    carried = {}
    for c in sorted(range(chunk_count), key=lambda i: -spread(i, tp_bits)):
        mask = spread(c, tp_bits)
        found = {r: swap_over(parts[r, c], "ep", r) if r else parts[r, c] for r in near}
        if not mask:
            found.update(gathered)
        total = combine(pick, found, carried.pop(mask, []))
        if mask:
            arrived = swap_over(total, "tp", low_bit(mask))
            carried.setdefault(mask ^ low_bit(mask), []).append(arrived)
    expert_out = total
    return (mixer_out, expert_out)


def solution(mesh):
    return jax.shard_map(
        local,
        mesh=mesh,
        in_specs=(
            P("ep", None),
            P("ep", None),
            P("ep", None),
            P(),
            P(),
            P(None, "tp"),
            P(None, "tp"),
            P(None, "tp"),
            P(None, "tp"),
            P("tp", None),
            P("ep", None),
            P(),
            P("ep", None),
            P("ep", None),
            P("ep", None, "tp"),
            P("ep", None, "tp"),
            P("ep", "tp", None),
        ),
        out_specs=(P(("ep", "tp"), None), P("ep", "tp")),
        check_vma=False,
    )
```

```python
import functools

import jax
import jax.numpy as jnp
from jax import lax
from jax.experimental import pallas as pl
from jax.experimental.pallas import tpu as pltpu
from jax.sharding import PartitionSpec as P


NOPE = 64
VDIM = 64
NORM_EPSILON = 1e-06
ROTARY_BASE = 10000.0
LOG2E = 1.4426950408889634

F32 = jnp.float32
BF16 = jnp.bfloat16

SMEM_SPEC = pl.BlockSpec(memory_space=pltpu.SMEM)
VMEM_SPEC = pl.BlockSpec(memory_space=pltpu.VMEM)
HBM_SPEC = pl.BlockSpec(memory_space=pltpu.HBM)


def in_hbm(value):
    return pltpu.with_memory_space_constraint(value, pltpu.HBM)


def params(mebibytes):
    return pltpu.CompilerParams(vmem_limit_bytes=mebibytes * 1024 * 1024)


def cost(flops, bytes_accessed):
    return pl.CostEstimate(
        flops=int(flops), bytes_accessed=int(bytes_accessed), transcendentals=0
    )


def swap_over(value, axis, mask):
    size = lax.axis_size(axis)
    return lax.ppermute(value, axis, [(i, i ^ mask) for i in range(size)])


def bits_of(size):
    return max(size - 1, 0).bit_length()


def spread(index, bits):
    return sum(((index >> (bits - 1 - b)) & 1) << b for b in range(bits))


def norm_value(source, gain):
    wide = source.astype(F32)
    factor = lax.rsqrt(jnp.mean(wide * wide, axis=-1, keepdims=True) + NORM_EPSILON)
    return (wide * factor * gain).astype(BF16)


def rotate_lanes(source, cosine, sine, half):
    width = source.shape[-1]
    lane = lax.broadcasted_iota(jnp.int32, source.shape, 1)
    first = (lane & (2 * half - 1)) < half
    partner = jnp.where(
        first, pltpu.roll(source, width - half, 1), pltpu.roll(source, half, 1)
    )
    return source * cosine + partner * sine


def prepare_kernel(
    ids, joint_hbm, joint_gain_hbm, rotary_hbm, routes_hbm, weights_hbm, rows_hbm, rows_gain_hbm,
    mine_hbm, other_hbm, meta_hbm, row_mine_hbm, row_other_hbm,
    joint, joint_gain, rotary, routes, weights, rows, rows_gain,
    mine, other, meta, row_mine, row_other, sems,
):
    inputs = (
        (joint_hbm, joint), (joint_gain_hbm, joint_gain), (rotary_hbm, rotary),
        (routes_hbm, routes), (weights_hbm, weights), (rows_gain_hbm, rows_gain), (rows_hbm, rows),
    )
    loads = [
        pltpu.make_async_copy(source, target, sems.at[i])
        for i, (source, target) in enumerate(inputs)
    ]
    outputs = (
        (mine, mine_hbm), (other, other_hbm), (meta, meta_hbm), (row_mine, row_mine_hbm),
        (row_other, row_other_hbm),
    )
    stores = [
        pltpu.make_async_copy(source, target, sems.at[len(loads) + i])
        for i, (source, target) in enumerate(outputs)
    ]
    for load in loads:
        load.start()
    for load in loads[:5]:
        load.wait()
    half, full = mine.shape
    count, width = joint.shape
    turn, top = rotary.shape[0], routes.shape[0]
    weight = weights[...]
    high = weight.astype(BF16).astype(F32)
    middle = (weight - high).astype(BF16).astype(F32)
    low = weight - high - middle
    rest = jnp.zeros((full - width - turn - 4 * top, count), F32)
    named = routes[...].astype(F32)
    meta[...] = jnp.concatenate([named, weight, rest[: 8 - 2 * top]], axis=0)
    side = jnp.concatenate(
        [rotary[...].astype(F32), named, high, middle, low, rest], axis=0
    ).T.astype(BF16)
    chosen = ids[1] == 0
    mine[:, width:] = jnp.where(chosen, side[:half], side[half:])
    other[:, width:] = jnp.where(chosen, side[half:], side[:half])
    own = pl.multiple_of(ids[1] * half, half)
    far = pl.multiple_of((1 - ids[1]) * half, half)
    mine[:, :width] = norm_value(joint[pl.ds(own, half), :], joint_gain[...])
    stores[0].start()
    other[:, :width] = norm_value(joint[pl.ds(far, half), :], joint_gain[...])
    stores[1].start()
    stores[2].start()
    for load in loads[5:]:
        load.wait()
    row_mine[...] = norm_value(rows[pl.ds(own, half), :], rows_gain[...])
    stores[3].start()
    row_other[...] = norm_value(rows[pl.ds(far, half), :], rows_gain[...])
    stores[4].start()
    for store in stores:
        store.wait()


def prepare(ids, joint, joint_gain, rotary, routes, weights, rows, rows_gain):
    count, width = joint.shape
    half = count // 2
    inputs = (
        joint, joint_gain.reshape(1, width), rotary.T, routes.T, weights.T, rows,
        rows_gain.reshape(1, rows.shape[1]),
    )
    outputs = (
        jax.ShapeDtypeStruct((half, width + 128), BF16),
        jax.ShapeDtypeStruct((half, width + 128), BF16),
        jax.ShapeDtypeStruct((8, count), F32),
        jax.ShapeDtypeStruct((half, rows.shape[1]), BF16),
        jax.ShapeDtypeStruct((half, rows.shape[1]), BF16),
    )
    return pl.pallas_call(
        prepare_kernel,
        out_shape=outputs,
        in_specs=[SMEM_SPEC] + [HBM_SPEC] * len(inputs),
        out_specs=(HBM_SPEC,) * len(outputs),
        scratch_shapes=[pltpu.VMEM(v.shape, v.dtype) for v in inputs + outputs]
        + [pltpu.SemaphoreType.DMA((len(inputs) + len(outputs),))],
        compiler_params=params(60),
        cost_estimate=cost(4e12 * 3e-6, 4e6),
        name="prepare",
    )(ids, *[in_hbm(v) for v in inputs])


def turn_tables(cosine, sine, start, count, lanes):
    turned = pl.ds(start, count)
    half = cosine.shape[0]
    repeat = lanes // (2 * half)
    c, s = cosine[:, turned], sine[:, turned]
    return (
        jnp.concatenate([c, c] * repeat, axis=0).T,
        jnp.concatenate([-s, s] * repeat, axis=0).T,
    )


def pick_value(local_count, capacity, group_count, ids, routes, out):
    tokens = routes.shape[1]
    group = ids[2]
    total = group_count * local_count
    row = lax.broadcasted_iota(jnp.int32, (total, tokens), 0)
    expert = ((group ^ (row // local_count)) * local_count + row % local_count)
    first = routes[0:1, :] == expert
    second = routes[1:2, :] == expert
    before = (
        lax.broadcasted_iota(jnp.int32, (tokens, tokens), 0)
        < lax.broadcasted_iota(jnp.int32, (tokens, tokens), 1)
    ).astype(BF16)
    named = jnp.where(first | second, 1.0, 0.0).astype(BF16)
    slot = jnp.dot(named, before, preferred_element_type=F32) + (row * capacity).astype(F32)
    pair = jnp.concatenate(
        [
            jnp.sum(jnp.where(first, slot, 0.0), axis=0, keepdims=True),
            jnp.sum(jnp.where(second, slot, 0.0), axis=0, keepdims=True),
            jnp.zeros((126, tokens), F32),
        ],
        axis=0,
    ).T
    span = 128
    for start in range(0, total * capacity, span):
        place = (lax.broadcasted_iota(jnp.int32, (tokens, span), 1) + start).astype(F32)
        out[:, start : start + span] = jnp.where(
            (place == pair[:, 0:1]) | (place == pair[:, 1:2]), 1.0, 0.0
        ).astype(BF16)


def query_kernel(
    turn_width, local_count, capacity, group_count, ids, query_latent, gain, query_weight,
    query_rotary, cosine, sine, routes, plain, turned, pick
):
    rows = query_latent.shape[0]
    normed = norm_value(query_latent[...], gain[...])
    plain[...] = jnp.dot(normed, query_weight[...], preferred_element_type=F32).astype(BF16)
    start = pl.multiple_of(ids[2] * rows, rows)
    c, s = turn_tables(cosine, sine, start, rows, turned.shape[1])
    turned[...] = rotate_lanes(
        jnp.dot(normed, query_rotary[...], preferred_element_type=F32), c, s, turn_width // 2
    ).astype(BF16)
    pick_value(local_count, capacity, group_count, ids, routes, pick)


def queries(
    ids, query_latent, gain, query_weight, query_rotary, cosine, sine, routes, turn_width,
    local_count, capacity, group_count,
):
    rows, width = query_latent.shape
    tokens = routes.shape[0]
    return pl.pallas_call(
        functools.partial(query_kernel, turn_width, local_count, capacity, group_count),
        out_shape=(
            jax.ShapeDtypeStruct((rows, query_weight.shape[1]), BF16),
            jax.ShapeDtypeStruct((rows, query_rotary.shape[1]), BF16),
            jax.ShapeDtypeStruct((tokens, group_count * local_count * capacity), BF16),
        ),
        in_specs=[SMEM_SPEC] + [VMEM_SPEC] * 7,
        out_specs=(VMEM_SPEC,) * 3,
        compiler_params=params(60),
        cost_estimate=cost(4e12 * 4e-6, 12e6),
        name="queries",
    )(
        ids, query_latent, gain.reshape(1, width), query_weight, query_rotary, cosine, sine,
        routes.T,
    )


def attention_kernel(
    turn_width, piece_count, tp_bits, ids, *rest
):
    sources = rest[:7]
    pieces = rest[7 : 7 + piece_count]
    keep, send, meta, keys, values, mixed = rest[7 + piece_count : 13 + piece_count]
    targets = rest[13 + piece_count : 20 + piece_count]
    sems = rest[-1]
    key_weight, value_weight, cosine, sine, plain, turned, output_weight = targets
    loads = [
        pltpu.make_async_copy(source, target, sems.at[i])
        for i, (source, target) in enumerate(zip(sources, targets))
    ]
    for load in loads:
        load.start()
    for load in loads[:4]:
        load.wait()
    rows = plain.shape[0]
    latent = key_weight.shape[0]
    turn_lanes = turned.shape[1]
    pair_count = keys.shape[0]
    pair = 2 * NOPE
    scale = LOG2E * (NOPE + turn_width) ** (-0.5)
    half = pieces[0].shape[0]
    repeat = turn_lanes // turn_width

    for index, piece in enumerate(pieces):
        name, side = index // 2, index % 2
        place = ids[1] if side == 0 else 1 - ids[1]
        base = pl.multiple_of(place * half, half)
        block = piece[:, :latent]
        start = index * half
        key_block = jnp.dot(block, key_weight[...], preferred_element_type=F32).astype(BF16)
        value_block = jnp.dot(block, value_weight[...], preferred_element_type=F32).astype(BF16)
        beside = piece[:, latent:].astype(F32)
        if name > 0:
            meta[name - 1, :, pl.ds(base, half)] = beside.T[turn_width : turn_width + 8, :]
        key = beside[:, :turn_width]
        key = jnp.concatenate([key] * repeat, axis=1)
        c, s = turn_tables(
            cosine, sine, pl.multiple_of(ids[3 + name] * rows + place * half, half), half,
            turn_lanes,
        )
        key = rotate_lanes(key, c, s, turn_width // 2).astype(BF16)
        for p in range(pair_count):
            keys[p, start : start + half, :pair] = key_block[:, p * pair : (p + 1) * pair]
            keys[p, start : start + half, pair:] = key
            values[p, start : start + half, :] = value_block[:, p * pair : (p + 1) * pair]

    loads[4].wait()
    loads[5].wait()
    tile = min(rows, 512)
    plain_lane = lax.broadcasted_iota(jnp.int32, (tile, pair), 1)
    turn_lane = lax.broadcasted_iota(jnp.int32, (tile, turn_lanes), 1)
    zero = jnp.zeros((), BF16)

    def step(index, carry):
        row = pl.ds(pl.multiple_of(index * tile, tile), tile)
        for p in range(pair_count):
            outs = []
            for h in range(2):
                head = 2 * p + h
                left = jnp.where(
                    (plain_lane // NOPE) == h, plain[row, p * pair : (p + 1) * pair], zero
                )
                right = jnp.where((turn_lane // turn_width) == head, turned[row, :], zero)
                query = jnp.concatenate([left, right], axis=1)
                scores = lax.dot_general(
                    query, keys[p], (((1,), (1,)), ((), ())), preferred_element_type=F32
                )
                top = jnp.max(scores, axis=1, keepdims=True)
                expo = jnp.exp2((scores - top) * scale)
                total = jnp.sum(expo, axis=1, keepdims=True)
                mix = jnp.dot(expo.astype(BF16), values[p], preferred_element_type=F32)
                outs.append(mix / total)
            mixed[row, p * pair : (p + 1) * pair] = jnp.where(
                plain_lane < VDIM, outs[0], outs[1]
            ).astype(BF16)
        return carry

    lax.fori_loop(0, rows // tile, step, 0)

    loads[6].wait()
    place_count = 1 << tp_bits
    block_rows = rows // place_count
    me = ids[0]
    middle = place_count // 2
    for target, low in ((send, middle), (keep, 0)):
        parts = [
            mixed[
                pl.ds(
                    pl.multiple_of((me ^ spread(low + i, tp_bits)) * block_rows, block_rows),
                    block_rows,
                ),
                :,
            ]
            for i in range(middle)
        ]
        target[...] = jnp.dot(
            jnp.concatenate(parts, axis=0), output_weight[...], preferred_element_type=F32
        ).astype(BF16)


def attention(
    ids, plain, turned, cosine, sine, key_weight, value_weight, output_weight, pieces,
    turn_width, tp_bits,
):
    rows = plain.shape[0]
    head_count = key_weight.shape[1] // NOPE
    key_rows = sum(p.shape[0] for p in pieces)
    sources = (key_weight, value_weight, cosine, sine, plain, turned, output_weight)
    turn_lanes = turned.shape[1]
    width = output_weight.shape[1]
    shape = jax.ShapeDtypeStruct((rows // 2, width), BF16)
    return pl.pallas_call(
        functools.partial(attention_kernel, turn_width, len(pieces), tp_bits),
        out_shape=(shape, shape, jax.ShapeDtypeStruct((len(pieces) // 2 - 1, 8, rows), F32)),
        in_specs=[SMEM_SPEC] + [HBM_SPEC] * 7 + [VMEM_SPEC] * len(pieces),
        out_specs=(VMEM_SPEC,) * 3,
        scratch_shapes=[
            pltpu.VMEM((head_count // 2, key_rows, 2 * NOPE + turn_lanes), BF16),
            pltpu.VMEM((head_count // 2, key_rows, 2 * VDIM), BF16),
            pltpu.VMEM((rows, head_count * VDIM), BF16),
        ]
        + [pltpu.VMEM(v.shape, v.dtype) for v in sources]
        + [
            pltpu.SemaphoreType.DMA((7,)),
        ],
        compiler_params=params(26 if key_rows <= 2048 else 60),
        cost_estimate=cost(4e12 * 12e-6, 40e6),
        name="attention",
    )(ids, *[in_hbm(v) for v in sources], *pieces)


def experts_kernel(
    names, fetch, group_count, capacity, tp_bits, ids, gate, up, down, *rest
):
    blocks = len(names)
    tables = rest[:blocks]
    pieces = rest[blocks : 3 * blocks]
    if fetch:
        sources = (gate, up, down)
        keep, send, gate, up, down, slots, loads, gathered, sems = rest[3 * blocks :]
        copies = [
            pltpu.make_async_copy(source.at[j], target.at[j], sems.at[3 * j + k])
            for j in range(gate.shape[0])
            for k, (source, target) in enumerate(zip(sources, (gate, up, down)))
        ]
        for copy in copies:
            copy.start()
    else:
        keep, send, slots, loads, gathered = rest[3 * blocks :]
    local_count = gate.shape[0]
    tokens = tables[0].shape[1]
    half = tokens // 2
    me, core, group = ids[0], ids[1], ids[2]

    before = (
        lax.broadcasted_iota(jnp.int32, (tokens, tokens), 0)
        < lax.broadcasted_iota(jnp.int32, (tokens, tokens), 1)
    ).astype(BF16)
    row = lax.broadcasted_iota(jnp.int32, (8, tokens), 0)
    wanted = (row + group * local_count).astype(F32)
    for b in range(blocks):
        meta = tables[b][...]
        first = meta[0:1, :] == wanted
        second = meta[1:2, :] == wanted
        named = (first | second) & (row < local_count)
        rank = jnp.dot(named.astype(BF16), before, preferred_element_type=F32)
        slots[b] = jnp.where(named, rank, -1.0)
        loads[b] = jnp.where(first, meta[2:3, :] + meta[4:5, :] + meta[6:7, :], 0.0) + jnp.where(
            second, meta[3:4, :] + meta[5:6, :] + meta[7:8, :], 0.0
        )

    own = pl.multiple_of(core * half, half)
    far = pl.multiple_of((1 - core) * half, half)
    place = lax.broadcasted_iota(jnp.int32, (capacity, half), 0).astype(F32)
    place_count = 1 << tp_bits
    part = down.shape[2] // place_count
    for j in range(local_count):
        scale = []
        for b in range(blocks):
            hits, weight = [], None
            for offset in (own, far):
                hit = place == slots[b, j : j + 1, pl.ds(offset, half)]
                load = jnp.where(hit, loads[b, j : j + 1, pl.ds(offset, half)], 0.0)
                load = jnp.sum(load, axis=1, keepdims=True)
                weight = load if weight is None else weight + load
                hits.append(jnp.where(hit, 1.0, 0.0).astype(BF16))
            block = jnp.concatenate([pieces[2 * b][...], pieces[2 * b + 1][...]], axis=0)
            gathered[b * capacity : (b + 1) * capacity, :] = jnp.dot(
                jnp.concatenate(hits, axis=1), block, preferred_element_type=F32
            ).astype(BF16)
            scale.append(weight)
        rows_in = gathered[...]
        if fetch:
            copies[3 * j].wait()
        gate_acts = jnp.dot(rows_in, gate[j], preferred_element_type=F32)
        if fetch:
            copies[3 * j + 1].wait()
        up_acts = jnp.dot(rows_in, up[j], preferred_element_type=F32)
        if fetch:
            copies[3 * j + 2].wait()
        hidden = (gate_acts * (1.0 / (1.0 + jnp.exp(-gate_acts))) * up_acts).astype(BF16)
        for target, low in ((send, place_count // 2), (keep, 0)):
            for i in range(place_count // 2):
                column = pl.multiple_of((me ^ spread(low + i, tp_bits)) * part, part)
                product = jnp.dot(
                    hidden, down[j, :, pl.ds(column, part)], preferred_element_type=F32
                )
                for b in range(blocks):
                    base = pl.multiple_of(
                        (ids[3 + group_count + names[b]] * local_count + j) * capacity, capacity
                    )
                    target[pl.ds(base, capacity), i * part : (i + 1) * part] = (
                        product[b * capacity : (b + 1) * capacity, :] * scale[b]
                    ).astype(BF16)


def run_experts(ids, group_count, names, tables, pieces, weights, fetch, capacity, tp_bits):
    local_count, width, _ = weights[0].shape
    count = len(names)
    tokens = tables[0].shape[1]
    rows = count * local_count * capacity
    shapes = [jax.ShapeDtypeStruct((rows, width // 2), BF16)] * 2
    scratch = [
        pltpu.VMEM((count, 8, tokens), F32),
        pltpu.VMEM((count, 8, tokens), F32),
        pltpu.VMEM((count * capacity, width), BF16),
    ]
    if fetch:
        shapes += [pltpu.VMEM(w.shape, w.dtype) for w in weights]
        scratch.append(pltpu.SemaphoreType.DMA((3 * local_count,)))
    return pl.pallas_call(
        functools.partial(
            experts_kernel, tuple(names), fetch, group_count, capacity, tp_bits
        ),
        out_shape=tuple(shapes),
        in_specs=[SMEM_SPEC]
        + [HBM_SPEC if fetch else VMEM_SPEC] * 3
        + [VMEM_SPEC] * (3 * count),
        out_specs=(VMEM_SPEC,) * len(shapes),
        scratch_shapes=scratch,
        compiler_params=params(24 if fetch else min(60, 18 + 4 * count)),
        cost_estimate=cost(4e12 * 5e-6 * count, 14e6 * count),
        name="experts",
    )(ids, *([in_hbm(w) for w in weights] if fetch else weights), *tables, *pieces)


def combine_kernel(starts, pick, *rest):
    out = rest[-1]
    count = len(starts)
    total = None
    for start, part in zip(starts, rest[:count]):
        span = part.shape[0]
        found = jnp.dot(pick[:, start : start + span], part[...], preferred_element_type=F32)
        total = found if total is None else total + found
    for carry in rest[count:-1]:
        total = total + carry[...].astype(F32)
    out[...] = total.astype(out.dtype)


def combine(pick, parts, carries, dtype):
    tokens = pick.shape[0]
    names = sorted(parts)
    span, width = parts[names[0]].shape
    operands = [parts[r] for r in names] + list(carries)
    return pl.pallas_call(
        functools.partial(combine_kernel, tuple(r * span for r in names)),
        out_shape=jax.ShapeDtypeStruct((tokens, width), dtype),
        in_specs=[VMEM_SPEC] * (1 + len(operands)),
        out_specs=VMEM_SPEC,
        compiler_params=params(24),
        cost_estimate=cost(4e12 * 1e-6, 4e6),
        name="combine",
    )(pick, *operands)


def low_bit(value):
    return value & -value


def reverse_bits(value, bits):
    return sum(((value >> b) & 1) << (bits - 1 - b) for b in range(bits))


def step_over(value, bit, ep_bits):
    groups, parts = lax.axis_size("ep"), lax.axis_size("tp")
    pairs = []
    for e in range(groups):
        for t in range(parts):
            mask = 1 << (bit if t % 2 == 0 else ep_bits - 1 - bit)
            pairs.append((e * parts + t, (e ^ mask) * parts + t))
    return lax.ppermute(value, ("ep", "tp"), pairs)


def add_wide(left, right):
    return (left.astype(F32) + right.astype(F32)).astype(BF16)


def local(
    query_latent,
    joint_latent,
    rotary_key,
    query_gain,
    joint_gain,
    query_weight,
    query_rotary,
    key_weight,
    value_weight,
    output_weight,
    expert_input,
    expert_gain,
    routes,
    route_weight,
    gate_weight,
    up_weight,
    down_weight,
):
    group_count = lax.axis_size("ep")
    part_count = lax.axis_size("tp")
    ep_bits, tp_bits = bits_of(group_count), bits_of(part_count)
    ep, tp = lax.axis_index("ep"), lax.axis_index("tp")
    core = tp & 1
    names = range(group_count)
    groups = [ep ^ jnp.where(core == 0, n, reverse_bits(n, ep_bits)) for n in names]
    direct = [n for n in names if bin(n).count("1") == 1]
    far = [n for n in names if bin(n).count("1") > 1]
    near = [0] + direct
    classes = [[0], direct] + ([far] if far else [])
    place = {n: c.index(n) for c in classes for n in c}
    orders = [jnp.where(core == 0, place[n], place[reverse_bits(n, ep_bits)]) for n in names]
    ids = jnp.stack([tp, core, ep] + groups + orders).astype(jnp.int32)
    rows = query_latent.shape[0]
    turn_width = rotary_key.shape[1]
    local_count = gate_weight.shape[0]
    tokens = expert_input.shape[0]
    capacity = 3 * tokens // (2 * group_count)
    half_width = turn_width // 2

    latent_mine, latent_other, own_meta, row_mine, row_other = prepare(
        ids, joint_latent, joint_gain, rotary_key, routes, route_weight, expert_input,
        expert_gain,
    )
    latent_held = {0: latent_mine}
    for b in range(ep_bits):
        latent_held[1 << b] = step_over(latent_mine, b, ep_bits)
    row_held = {0: row_mine, 1: step_over(row_mine, 0, ep_bits)}

    positions = jnp.arange(rows * group_count, dtype=jnp.int32).astype(F32)
    frequencies = ROTARY_BASE ** (-jnp.arange(half_width, dtype=F32) / half_width)
    angles = frequencies[:, None] * positions[None, :]
    cosine, sine = jnp.cos(angles), jnp.sin(angles)
    plain, turned, pick = queries(
        ids, query_latent, query_gain, query_weight, query_rotary, cosine,
        sine, routes, turn_width, local_count, capacity, group_count,
    )
    for n in far:
        b = n.bit_length() - 1
        latent_held[n] = step_over(latent_held[n ^ (1 << b)], b, ep_bits)
    own_keep, own_send, *weights = run_experts(
        ids, group_count, [0], [own_meta], [row_mine, row_other],
        (gate_weight, up_weight, down_weight), True, capacity, tp_bits,
    )

    for b in range(1, ep_bits):
        row_held[1 << b] = step_over(row_mine, b, ep_bits)

    def with_other(values, own_other):
        swapped = {n: swap_over(values[n], "tp", 1) for n in names if n}
        return {
            n: [values[n], swapped[reverse_bits(n, ep_bits)] if n else own_other] for n in names
        }

    latents = with_other(latent_held, latent_other)
    keep, send, metas = attention(
        ids, plain, turned, cosine, sine, key_weight, value_weight, output_weight,
        [piece for n in names for piece in latents[n]], turn_width, tp_bits,
    )
    for n in far:
        b = n.bit_length() - 1
        row_held[n] = step_over(row_held[n ^ (1 << b)], b, ep_bits)
    arrived = swap_over(send, "tp", 1)
    for b in range(1, tp_bits):
        cut = keep.shape[0] // 2
        away = add_wide(keep[cut:], arrived[cut:])
        keep = add_wide(keep[:cut], arrived[:cut])
        arrived = swap_over(away, "tp", 1 << b)
    mixer_out = add_wide(keep, arrived)

    row_pairs = with_other(row_held, row_other)
    parts = {}
    span = local_count * capacity
    chunk_count = part_count // 2
    width = expert_input.shape[1] // part_count
    gathered = {}
    for chosen in classes:
        if chosen == [0]:
            keep, send = own_keep, own_send
        else:
            keep, send = run_experts(
                ids, group_count, chosen, [metas[n - 1] for n in chosen],
                [piece for n in chosen for piece in row_pairs[n]], weights, False,
                capacity, tp_bits,
            )
        arrived = swap_over(send, "tp", 1)
        if chosen != far:
            both = add_wide(keep, arrived)
            for i, r in enumerate(chosen):
                for c in range(chunk_count):
                    parts[r, c] = both[i * span : (i + 1) * span, c * width : (c + 1) * width]
        else:
            for b in range(1, tp_bits):
                cut = keep.shape[1] // 2
                away = add_wide(keep[:, cut:], arrived[:, cut:])
                keep = add_wide(keep[:, :cut], arrived[:, :cut])
                arrived = swap_over(away, "tp", 1 << b)
            both = add_wide(keep, arrived)
            for i, r in enumerate(chosen):
                gathered[r] = swap_over(both[i * span : (i + 1) * span], "ep", r)

    carried = {}
    for c in sorted(range(chunk_count), key=lambda i: -spread(i, tp_bits)):
        mask = spread(c, tp_bits)
        found = {r: swap_over(parts[r, c], "ep", r) if r else parts[r, c] for r in near}
        if not mask:
            found.update(gathered)
        carries = carried.pop(mask, [])
        if mask:
            total = combine(pick, found, carries, BF16)
        else:
            total = combine(pick, found, [], F32)
        if mask:
            arrived = swap_over(total, "tp", low_bit(mask))
            carried.setdefault(mask ^ low_bit(mask), []).append(arrived)
    for carry in carries:
        total = total + carry.astype(F32)
    expert_out = total.astype(BF16)
    return (mixer_out, expert_out)


def solution(mesh):
    return jax.shard_map(
        local,
        mesh=mesh,
        in_specs=(
            P("ep", None),
            P("ep", None),
            P("ep", None),
            P(),
            P(),
            P(None, "tp"),
            P(None, "tp"),
            P(None, "tp"),
            P(None, "tp"),
            P("tp", None),
            P("ep", None),
            P(),
            P("ep", None),
            P("ep", None),
            P("ep", None, "tp"),
            P("ep", None, "tp"),
            P("ep", "tp", None),
        ),
        out_specs=(P(("ep", "tp"), None), P("ep", "tp")),
        check_vma=False,
    )
```

```python
import functools

import jax
import jax.numpy as jnp
from jax import lax
from jax.experimental import pallas as pl
from jax.experimental.pallas import tpu as pltpu
from jax.sharding import PartitionSpec as P


NOPE = 64
VDIM = 64
NORM_EPSILON = 1e-06
ROTARY_BASE = 10000.0
LOG2E = 1.4426950408889634

F32 = jnp.float32
BF16 = jnp.bfloat16

SMEM_SPEC = pl.BlockSpec(memory_space=pltpu.SMEM)
VMEM_SPEC = pl.BlockSpec(memory_space=pltpu.VMEM)
HBM_SPEC = pl.BlockSpec(memory_space=pltpu.HBM)


def in_hbm(value):
    return pltpu.with_memory_space_constraint(value, pltpu.HBM)


def params(mebibytes):
    return pltpu.CompilerParams(vmem_limit_bytes=mebibytes * 1024 * 1024)


def cost(flops, bytes_accessed):
    return pl.CostEstimate(
        flops=int(flops), bytes_accessed=int(bytes_accessed), transcendentals=0
    )


def swap_over(value, axis, mask):
    size = lax.axis_size(axis)
    return lax.ppermute(value, axis, [(i, i ^ mask) for i in range(size)])


def bits_of(size):
    return max(size - 1, 0).bit_length()


def spread(index, bits):
    return sum(((index >> (bits - 1 - b)) & 1) << b for b in range(bits))


def norm_value(source, gain):
    wide = source.astype(F32)
    factor = lax.rsqrt(jnp.mean(wide * wide, axis=-1, keepdims=True) + NORM_EPSILON)
    return (wide * factor * gain).astype(BF16)


def rotate_lanes(source, cosine, sine, half):
    width = source.shape[-1]
    lane = lax.broadcasted_iota(jnp.int32, source.shape, 1)
    first = (lane & (2 * half - 1)) < half
    partner = jnp.where(
        first, pltpu.roll(source, width - half, 1), pltpu.roll(source, half, 1)
    )
    return source * cosine + partner * sine


def prepare_kernel(
    ids, joint_hbm, joint_gain_hbm, rotary_hbm, routes_hbm, weights_hbm, rows_hbm, rows_gain_hbm,
    mine_hbm, other_hbm, meta_hbm, row_mine_hbm, row_other_hbm,
    joint, joint_gain, rotary, routes, weights, rows, rows_gain,
    mine, other, meta, row_mine, row_other, sems,
):
    inputs = (
        (joint_hbm, joint), (joint_gain_hbm, joint_gain), (rotary_hbm, rotary),
        (routes_hbm, routes), (weights_hbm, weights), (rows_gain_hbm, rows_gain), (rows_hbm, rows),
    )
    half, full = mine.shape
    own = pl.multiple_of(ids[1] * half, half)
    far = pl.multiple_of((1 - ids[1]) * half, half)
    cut = half // 2
    spans = [(own, 0), (own, cut), (far, 0), (far, cut)]
    inputs = inputs[:-1] + tuple(
        (rows_hbm.at[pl.ds(base + at, cut)], rows.at[pl.ds(base + at, cut)]) for base, at in spans
    )
    loads = [
        pltpu.make_async_copy(source, target, sems.at[i])
        for i, (source, target) in enumerate(inputs)
    ]
    outputs = ((mine, mine_hbm), (other, other_hbm), (meta, meta_hbm)) + tuple(
        (source.at[pl.ds(at, cut)], target.at[pl.ds(at, cut)])
        for (source, target), (_, at) in zip(
            [(row_mine, row_mine_hbm)] * 2 + [(row_other, row_other_hbm)] * 2, spans
        )
    )
    stores = [
        pltpu.make_async_copy(source, target, sems.at[len(loads) + i])
        for i, (source, target) in enumerate(outputs)
    ]
    for load in loads:
        load.start()
    for load in loads[:5]:
        load.wait()
    count, width = joint.shape
    turn, top = rotary.shape[0], routes.shape[0]
    weight = weights[...]
    high = weight.astype(BF16).astype(F32)
    middle = (weight - high).astype(BF16).astype(F32)
    low = weight - high - middle
    rest = jnp.zeros((full - width - turn - 4 * top, count), F32)
    named = routes[...].astype(F32)
    meta[...] = jnp.concatenate([named, weight, rest[: 8 - 2 * top]], axis=0)
    side = jnp.concatenate(
        [rotary[...].astype(F32), named, high, middle, low, rest], axis=0
    ).T.astype(BF16)
    chosen = ids[1] == 0
    mine[:, width:] = jnp.where(chosen, side[:half], side[half:])
    other[:, width:] = jnp.where(chosen, side[half:], side[:half])
    mine[:, :width] = norm_value(joint[pl.ds(own, half), :], joint_gain[...])
    stores[0].start()
    other[:, :width] = norm_value(joint[pl.ds(far, half), :], joint_gain[...])
    stores[1].start()
    stores[2].start()
    loads[5].wait()
    for i, (base, at) in enumerate(spans):
        loads[6 + i].wait()
        target = row_mine if i < 2 else row_other
        target[at : at + cut, :] = norm_value(rows[pl.ds(base + at, cut), :], rows_gain[...])
        stores[3 + i].start()
    for store in stores:
        store.wait()


def prepare(ids, joint, joint_gain, rotary, routes, weights, rows, rows_gain):
    count, width = joint.shape
    half = count // 2
    inputs = (
        joint, joint_gain.reshape(1, width), rotary.T, routes.T, weights.T, rows,
        rows_gain.reshape(1, rows.shape[1]),
    )
    outputs = (
        jax.ShapeDtypeStruct((half, width + 128), BF16),
        jax.ShapeDtypeStruct((half, width + 128), BF16),
        jax.ShapeDtypeStruct((8, count), F32),
        jax.ShapeDtypeStruct((half, rows.shape[1]), BF16),
        jax.ShapeDtypeStruct((half, rows.shape[1]), BF16),
    )
    return pl.pallas_call(
        prepare_kernel,
        out_shape=outputs,
        in_specs=[SMEM_SPEC] + [HBM_SPEC] * len(inputs),
        out_specs=(HBM_SPEC,) * len(outputs),
        scratch_shapes=[pltpu.VMEM(v.shape, v.dtype) for v in inputs + outputs]
        + [pltpu.SemaphoreType.DMA((len(inputs) + len(outputs) + 5,))],
        compiler_params=params(60),
        cost_estimate=cost(4e12 * 3e-6, 4e6),
        name="prepare",
    )(ids, *[in_hbm(v) for v in inputs])


def turn_tables(cosine, sine, start, count, lanes):
    turned = pl.ds(start, count)
    half = cosine.shape[0]
    repeat = lanes // (2 * half)
    c, s = cosine[:, turned], sine[:, turned]
    return (
        jnp.concatenate([c, c] * repeat, axis=0).T,
        jnp.concatenate([-s, s] * repeat, axis=0).T,
    )


def pick_value(local_count, capacity, group_count, ids, routes, out):
    tokens = routes.shape[1]
    group = ids[2]
    total = group_count * local_count
    row = lax.broadcasted_iota(jnp.int32, (total, tokens), 0)
    expert = ((group ^ (row // local_count)) * local_count + row % local_count)
    first = routes[0:1, :] == expert
    second = routes[1:2, :] == expert
    before = (
        lax.broadcasted_iota(jnp.int32, (tokens, tokens), 0)
        < lax.broadcasted_iota(jnp.int32, (tokens, tokens), 1)
    ).astype(BF16)
    named = jnp.where(first | second, 1.0, 0.0).astype(BF16)
    slot = jnp.dot(named, before, preferred_element_type=F32) + (row * capacity).astype(F32)
    pair = jnp.concatenate(
        [
            jnp.sum(jnp.where(first, slot, 0.0), axis=0, keepdims=True),
            jnp.sum(jnp.where(second, slot, 0.0), axis=0, keepdims=True),
            jnp.zeros((126, tokens), F32),
        ],
        axis=0,
    ).T
    span = 128
    for start in range(0, total * capacity, span):
        place = (lax.broadcasted_iota(jnp.int32, (tokens, span), 1) + start).astype(F32)
        out[:, start : start + span] = jnp.where(
            (place == pair[:, 0:1]) | (place == pair[:, 1:2]), 1.0, 0.0
        ).astype(BF16)


def query_kernel(
    turn_width, local_count, capacity, group_count, ids, query_latent, gain, query_weight,
    query_rotary, cosine, sine, routes, plain, turned, pick
):
    rows = query_latent.shape[0]
    normed = norm_value(query_latent[...], gain[...])
    plain[...] = jnp.dot(normed, query_weight[...], preferred_element_type=F32).astype(BF16)
    start = pl.multiple_of(ids[2] * rows, rows)
    c, s = turn_tables(cosine, sine, start, rows, turned.shape[1])
    turned[...] = rotate_lanes(
        jnp.dot(normed, query_rotary[...], preferred_element_type=F32), c, s, turn_width // 2
    ).astype(BF16)
    pick_value(local_count, capacity, group_count, ids, routes, pick)


def queries(
    ids, query_latent, gain, query_weight, query_rotary, cosine, sine, routes, turn_width,
    local_count, capacity, group_count,
):
    rows, width = query_latent.shape
    tokens = routes.shape[0]
    return pl.pallas_call(
        functools.partial(query_kernel, turn_width, local_count, capacity, group_count),
        out_shape=(
            jax.ShapeDtypeStruct((rows, query_weight.shape[1]), BF16),
            jax.ShapeDtypeStruct((rows, query_rotary.shape[1]), BF16),
            jax.ShapeDtypeStruct((tokens, group_count * local_count * capacity), BF16),
        ),
        in_specs=[SMEM_SPEC] + [VMEM_SPEC] * 7,
        out_specs=(VMEM_SPEC,) * 3,
        compiler_params=params(60),
        cost_estimate=cost(4e12 * 4e-6, 12e6),
        name="queries",
    )(
        ids, query_latent, gain.reshape(1, width), query_weight, query_rotary, cosine, sine,
        routes.T,
    )


def attention_kernel(
    turn_width, piece_count, tp_bits, ids, *rest
):
    sources = rest[:7]
    pieces = rest[7 : 7 + piece_count]
    keep, send, meta, keys, values, mixed = rest[7 + piece_count : 13 + piece_count]
    targets = rest[13 + piece_count : 20 + piece_count]
    sems = rest[-1]
    key_weight, value_weight, cosine, sine, plain, turned, output_weight = targets
    loads = [
        pltpu.make_async_copy(source, target, sems.at[i])
        for i, (source, target) in enumerate(zip(sources, targets))
    ]
    for load in loads:
        load.start()
    for load in loads[:4]:
        load.wait()
    rows = plain.shape[0]
    latent = key_weight.shape[0]
    turn_lanes = turned.shape[1]
    pair_count = keys.shape[0]
    pair = 2 * NOPE
    scale = LOG2E * (NOPE + turn_width) ** (-0.5)
    half = pieces[0].shape[0]
    repeat = turn_lanes // turn_width

    for index, piece in enumerate(pieces):
        name, side = index // 2, index % 2
        place = ids[1] if side == 0 else 1 - ids[1]
        base = pl.multiple_of(place * half, half)
        block = piece[:, :latent]
        start = index * half
        key_block = jnp.dot(block, key_weight[...], preferred_element_type=F32).astype(BF16)
        value_block = jnp.dot(block, value_weight[...], preferred_element_type=F32).astype(BF16)
        beside = piece[:, latent:].astype(F32)
        if name > 0:
            meta[name - 1, :, pl.ds(base, half)] = beside.T[turn_width : turn_width + 8, :]
        key = beside[:, :turn_width]
        key = jnp.concatenate([key] * repeat, axis=1)
        c, s = turn_tables(
            cosine, sine, pl.multiple_of(ids[3 + name] * rows + place * half, half), half,
            turn_lanes,
        )
        key = rotate_lanes(key, c, s, turn_width // 2).astype(BF16)
        for p in range(pair_count):
            keys[p, start : start + half, :pair] = key_block[:, p * pair : (p + 1) * pair]
            keys[p, start : start + half, pair:] = key
            values[p, start : start + half, :] = value_block[:, p * pair : (p + 1) * pair]

    loads[4].wait()
    loads[5].wait()
    tile = min(rows, 512)
    plain_lane = lax.broadcasted_iota(jnp.int32, (tile, pair), 1)
    turn_lane = lax.broadcasted_iota(jnp.int32, (tile, turn_lanes), 1)
    zero = jnp.zeros((), BF16)

    def step(index, carry):
        row = pl.ds(pl.multiple_of(index * tile, tile), tile)
        for p in range(pair_count):
            outs = []
            for h in range(2):
                head = 2 * p + h
                left = jnp.where(
                    (plain_lane // NOPE) == h, plain[row, p * pair : (p + 1) * pair], zero
                )
                right = jnp.where((turn_lane // turn_width) == head, turned[row, :], zero)
                query = jnp.concatenate([left, right], axis=1)
                scores = lax.dot_general(
                    query, keys[p], (((1,), (1,)), ((), ())), preferred_element_type=F32
                )
                top = jnp.max(scores, axis=1, keepdims=True)
                expo = jnp.exp2((scores - top) * scale)
                total = jnp.sum(expo, axis=1, keepdims=True)
                mix = jnp.dot(expo.astype(BF16), values[p], preferred_element_type=F32)
                outs.append(mix / total)
            mixed[row, p * pair : (p + 1) * pair] = jnp.where(
                plain_lane < VDIM, outs[0], outs[1]
            ).astype(BF16)
        return carry

    lax.fori_loop(0, rows // tile, step, 0)

    loads[6].wait()
    place_count = 1 << tp_bits
    block_rows = rows // place_count
    me = ids[0]
    middle = place_count // 2
    for target, low in ((send, middle), (keep, 0)):
        parts = [
            mixed[
                pl.ds(
                    pl.multiple_of((me ^ spread(low + i, tp_bits)) * block_rows, block_rows),
                    block_rows,
                ),
                :,
            ]
            for i in range(middle)
        ]
        target[...] = jnp.dot(
            jnp.concatenate(parts, axis=0), output_weight[...], preferred_element_type=F32
        ).astype(BF16)


def attention(
    ids, plain, turned, cosine, sine, key_weight, value_weight, output_weight, pieces,
    turn_width, tp_bits,
):
    rows = plain.shape[0]
    head_count = key_weight.shape[1] // NOPE
    key_rows = sum(p.shape[0] for p in pieces)
    sources = (key_weight, value_weight, cosine, sine, plain, turned, output_weight)
    turn_lanes = turned.shape[1]
    width = output_weight.shape[1]
    shape = jax.ShapeDtypeStruct((rows // 2, width), BF16)
    return pl.pallas_call(
        functools.partial(attention_kernel, turn_width, len(pieces), tp_bits),
        out_shape=(shape, shape, jax.ShapeDtypeStruct((len(pieces) // 2 - 1, 8, rows), F32)),
        in_specs=[SMEM_SPEC] + [HBM_SPEC] * 7 + [VMEM_SPEC] * len(pieces),
        out_specs=(VMEM_SPEC,) * 3,
        scratch_shapes=[
            pltpu.VMEM((head_count // 2, key_rows, 2 * NOPE + turn_lanes), BF16),
            pltpu.VMEM((head_count // 2, key_rows, 2 * VDIM), BF16),
            pltpu.VMEM((rows, head_count * VDIM), BF16),
        ]
        + [pltpu.VMEM(v.shape, v.dtype) for v in sources]
        + [
            pltpu.SemaphoreType.DMA((7,)),
        ],
        compiler_params=params(26 if key_rows <= 2048 else 60),
        cost_estimate=cost(4e12 * 12e-6, 40e6),
        name="attention",
    )(ids, *[in_hbm(v) for v in sources], *pieces)


def experts_kernel(
    names, fetch, group_count, capacity, tp_bits, ids, gate, up, down, *rest
):
    blocks = len(names)
    tables = rest[:blocks]
    pieces = rest[blocks : 3 * blocks]
    if fetch:
        sources = (gate, up, down)
        keep, send, gate, up, down, slots, loads, gathered, sems = rest[3 * blocks :]
        copies = [
            pltpu.make_async_copy(source.at[j], target.at[j], sems.at[3 * j + k])
            for j in range(gate.shape[0])
            for k, (source, target) in enumerate(zip(sources, (gate, up, down)))
        ]
        for copy in copies:
            copy.start()
    else:
        keep, send, slots, loads, gathered = rest[3 * blocks :]
    local_count = gate.shape[0]
    tokens = tables[0].shape[1]
    half = tokens // 2
    me, core, group = ids[0], ids[1], ids[2]

    before = (
        lax.broadcasted_iota(jnp.int32, (tokens, tokens), 0)
        < lax.broadcasted_iota(jnp.int32, (tokens, tokens), 1)
    ).astype(BF16)
    row = lax.broadcasted_iota(jnp.int32, (8, tokens), 0)
    wanted = (row + group * local_count).astype(F32)
    for b in range(blocks):
        meta = tables[b][...]
        first = meta[0:1, :] == wanted
        second = meta[1:2, :] == wanted
        named = (first | second) & (row < local_count)
        rank = jnp.dot(named.astype(BF16), before, preferred_element_type=F32)
        slots[b] = jnp.where(named, rank, -1.0)
        loads[b] = jnp.where(first, meta[2:3, :] + meta[4:5, :] + meta[6:7, :], 0.0) + jnp.where(
            second, meta[3:4, :] + meta[5:6, :] + meta[7:8, :], 0.0
        )

    own = pl.multiple_of(core * half, half)
    far = pl.multiple_of((1 - core) * half, half)
    place = lax.broadcasted_iota(jnp.int32, (capacity, half), 0).astype(F32)
    place_count = 1 << tp_bits
    part = down.shape[2] // place_count
    for j in range(local_count):
        scale = []
        for b in range(blocks):
            hits, weight = [], None
            for offset in (own, far):
                hit = place == slots[b, j : j + 1, pl.ds(offset, half)]
                load = jnp.where(hit, loads[b, j : j + 1, pl.ds(offset, half)], 0.0)
                load = jnp.sum(load, axis=1, keepdims=True)
                weight = load if weight is None else weight + load
                hits.append(jnp.where(hit, 1.0, 0.0).astype(BF16))
            block = jnp.concatenate([pieces[2 * b][...], pieces[2 * b + 1][...]], axis=0)
            gathered[b * capacity : (b + 1) * capacity, :] = jnp.dot(
                jnp.concatenate(hits, axis=1), block, preferred_element_type=F32
            ).astype(BF16)
            scale.append(weight)
        rows_in = gathered[...]
        if fetch:
            copies[3 * j].wait()
        gate_acts = jnp.dot(rows_in, gate[j], preferred_element_type=F32)
        if fetch:
            copies[3 * j + 1].wait()
        up_acts = jnp.dot(rows_in, up[j], preferred_element_type=F32)
        if fetch:
            copies[3 * j + 2].wait()
        hidden = (gate_acts * (1.0 / (1.0 + jnp.exp(-gate_acts))) * up_acts).astype(BF16)
        for target, low in ((send, place_count // 2), (keep, 0)):
            for i in range(place_count // 2):
                column = pl.multiple_of((me ^ spread(low + i, tp_bits)) * part, part)
                product = jnp.dot(
                    hidden, down[j, :, pl.ds(column, part)], preferred_element_type=F32
                )
                for b in range(blocks):
                    base = pl.multiple_of(
                        (ids[3 + group_count + names[b]] * local_count + j) * capacity, capacity
                    )
                    target[pl.ds(base, capacity), i * part : (i + 1) * part] = (
                        product[b * capacity : (b + 1) * capacity, :] * scale[b]
                    ).astype(BF16)


def run_experts(ids, group_count, names, tables, pieces, weights, fetch, capacity, tp_bits):
    local_count, width, _ = weights[0].shape
    count = len(names)
    tokens = tables[0].shape[1]
    rows = count * local_count * capacity
    shapes = [jax.ShapeDtypeStruct((rows, width // 2), BF16)] * 2
    scratch = [
        pltpu.VMEM((count, 8, tokens), F32),
        pltpu.VMEM((count, 8, tokens), F32),
        pltpu.VMEM((count * capacity, width), BF16),
    ]
    if fetch:
        shapes += [pltpu.VMEM(w.shape, w.dtype) for w in weights]
        scratch.append(pltpu.SemaphoreType.DMA((3 * local_count,)))
    return pl.pallas_call(
        functools.partial(
            experts_kernel, tuple(names), fetch, group_count, capacity, tp_bits
        ),
        out_shape=tuple(shapes),
        in_specs=[SMEM_SPEC]
        + [HBM_SPEC if fetch else VMEM_SPEC] * 3
        + [VMEM_SPEC] * (3 * count),
        out_specs=(VMEM_SPEC,) * len(shapes),
        scratch_shapes=scratch,
        compiler_params=params(24 if fetch else min(60, 18 + 4 * count)),
        cost_estimate=cost(4e12 * 5e-6 * count, 14e6 * count),
        name="experts",
    )(ids, *([in_hbm(w) for w in weights] if fetch else weights), *tables, *pieces)


def combine_kernel(starts, pick, *rest):
    out = rest[-1]
    count = len(starts)
    total = None
    for start, part in zip(starts, rest[:count]):
        span = part.shape[0]
        found = jnp.dot(pick[:, start : start + span], part[...], preferred_element_type=F32)
        total = found if total is None else total + found
    for carry in rest[count:-1]:
        total = total + carry[...].astype(F32)
    out[...] = total.astype(out.dtype)


def combine(pick, parts, carries, dtype):
    tokens = pick.shape[0]
    names = sorted(parts)
    span, width = parts[names[0]].shape
    operands = [parts[r] for r in names] + list(carries)
    return pl.pallas_call(
        functools.partial(combine_kernel, tuple(r * span for r in names)),
        out_shape=jax.ShapeDtypeStruct((tokens, width), dtype),
        in_specs=[VMEM_SPEC] * (1 + len(operands)),
        out_specs=VMEM_SPEC,
        compiler_params=params(24),
        cost_estimate=cost(4e12 * 1e-6, 4e6),
        name="combine",
    )(pick, *operands)


def low_bit(value):
    return value & -value


def reverse_bits(value, bits):
    return sum(((value >> b) & 1) << (bits - 1 - b) for b in range(bits))


def step_over(value, bit, ep_bits):
    groups, parts = lax.axis_size("ep"), lax.axis_size("tp")
    pairs = []
    for e in range(groups):
        for t in range(parts):
            mask = 1 << (bit if t % 2 == 0 else ep_bits - 1 - bit)
            pairs.append((e * parts + t, (e ^ mask) * parts + t))
    return lax.ppermute(value, ("ep", "tp"), pairs)


def add_wide(left, right):
    return (left.astype(F32) + right.astype(F32)).astype(BF16)


def local(
    query_latent,
    joint_latent,
    rotary_key,
    query_gain,
    joint_gain,
    query_weight,
    query_rotary,
    key_weight,
    value_weight,
    output_weight,
    expert_input,
    expert_gain,
    routes,
    route_weight,
    gate_weight,
    up_weight,
    down_weight,
):
    group_count = lax.axis_size("ep")
    part_count = lax.axis_size("tp")
    ep_bits, tp_bits = bits_of(group_count), bits_of(part_count)
    ep, tp = lax.axis_index("ep"), lax.axis_index("tp")
    core = tp & 1
    names = range(group_count)
    groups = [ep ^ jnp.where(core == 0, n, reverse_bits(n, ep_bits)) for n in names]
    direct = [n for n in names if bin(n).count("1") == 1]
    far = [n for n in names if bin(n).count("1") > 1]
    near = [0] + direct
    classes = [[0], direct] + ([far] if far else [])
    place = {n: c.index(n) for c in classes for n in c}
    orders = [jnp.where(core == 0, place[n], place[reverse_bits(n, ep_bits)]) for n in names]
    ids = jnp.stack([tp, core, ep] + groups + orders).astype(jnp.int32)
    rows = query_latent.shape[0]
    turn_width = rotary_key.shape[1]
    local_count = gate_weight.shape[0]
    tokens = expert_input.shape[0]
    capacity = 3 * tokens // (2 * group_count)
    half_width = turn_width // 2

    latent_mine, latent_other, own_meta, row_mine, row_other = prepare(
        ids, joint_latent, joint_gain, rotary_key, routes, route_weight, expert_input,
        expert_gain,
    )
    latent_held = {0: latent_mine}
    for b in range(ep_bits):
        latent_held[1 << b] = step_over(latent_mine, b, ep_bits)
    row_held = {0: row_mine, 1: step_over(row_mine, 0, ep_bits)}

    positions = jnp.arange(rows * group_count, dtype=jnp.int32).astype(F32)
    frequencies = ROTARY_BASE ** (-jnp.arange(half_width, dtype=F32) / half_width)
    angles = frequencies[:, None] * positions[None, :]
    cosine, sine = jnp.cos(angles), jnp.sin(angles)
    plain, turned, pick = queries(
        ids, query_latent, query_gain, query_weight, query_rotary, cosine,
        sine, routes, turn_width, local_count, capacity, group_count,
    )
    for n in far:
        b = n.bit_length() - 1
        latent_held[n] = step_over(latent_held[n ^ (1 << b)], b, ep_bits)
    own_keep, own_send, *weights = run_experts(
        ids, group_count, [0], [own_meta], [row_mine, row_other],
        (gate_weight, up_weight, down_weight), True, capacity, tp_bits,
    )

    for b in range(1, ep_bits):
        row_held[1 << b] = step_over(row_mine, b, ep_bits)

    def with_other(values, own_other):
        swapped = {n: swap_over(values[n], "tp", 1) for n in names if n}
        return {
            n: [values[n], swapped[reverse_bits(n, ep_bits)] if n else own_other] for n in names
        }

    latents = with_other(latent_held, latent_other)
    keep, send, metas = attention(
        ids, plain, turned, cosine, sine, key_weight, value_weight, output_weight,
        [piece for n in names for piece in latents[n]], turn_width, tp_bits,
    )
    for n in far:
        b = n.bit_length() - 1
        row_held[n] = step_over(row_held[n ^ (1 << b)], b, ep_bits)
    arrived = swap_over(send, "tp", 1)
    for b in range(1, tp_bits):
        cut = keep.shape[0] // 2
        away = add_wide(keep[cut:], arrived[cut:])
        keep = add_wide(keep[:cut], arrived[:cut])
        arrived = swap_over(away, "tp", 1 << b)
    mixer_out = add_wide(keep, arrived)

    row_pairs = with_other(row_held, row_other)
    parts = {}
    span = local_count * capacity
    chunk_count = part_count // 2
    width = expert_input.shape[1] // part_count
    gathered = {}
    for chosen in classes:
        if chosen == [0]:
            keep, send = own_keep, own_send
        else:
            keep, send = run_experts(
                ids, group_count, chosen, [metas[n - 1] for n in chosen],
                [piece for n in chosen for piece in row_pairs[n]], weights, False,
                capacity, tp_bits,
            )
        arrived = swap_over(send, "tp", 1)
        if chosen != far:
            both = add_wide(keep, arrived)
            for i, r in enumerate(chosen):
                for c in range(chunk_count):
                    parts[r, c] = both[i * span : (i + 1) * span, c * width : (c + 1) * width]
        else:
            for b in range(1, tp_bits):
                cut = keep.shape[1] // 2
                away = add_wide(keep[:, cut:], arrived[:, cut:])
                keep = add_wide(keep[:, :cut], arrived[:, :cut])
                arrived = swap_over(away, "tp", 1 << b)
            both = add_wide(keep, arrived)
            for i, r in enumerate(chosen):
                gathered[r] = swap_over(both[i * span : (i + 1) * span], "ep", r)

    carried = {}
    for c in sorted(range(chunk_count), key=lambda i: -spread(i, tp_bits)):
        mask = spread(c, tp_bits)
        found = {r: swap_over(parts[r, c], "ep", r) if r else parts[r, c] for r in near}
        if not mask:
            found.update(gathered)
        carries = carried.pop(mask, [])
        if mask:
            total = combine(pick, found, carries, BF16)
        else:
            total = combine(pick, found, [], F32)
        if mask:
            arrived = swap_over(total, "tp", low_bit(mask))
            carried.setdefault(mask ^ low_bit(mask), []).append(arrived)
    for carry in carries:
        total = total + carry.astype(F32)
    expert_out = total.astype(BF16)
    return (mixer_out, expert_out)


def solution(mesh):
    return jax.shard_map(
        local,
        mesh=mesh,
        in_specs=(
            P("ep", None),
            P("ep", None),
            P("ep", None),
            P(),
            P(),
            P(None, "tp"),
            P(None, "tp"),
            P(None, "tp"),
            P(None, "tp"),
            P("tp", None),
            P("ep", None),
            P(),
            P("ep", None),
            P("ep", None),
            P("ep", None, "tp"),
            P("ep", None, "tp"),
            P("ep", "tp", None),
        ),
        out_specs=(P(("ep", "tp"), None), P("ep", "tp")),
        check_vma=False,
    )
```
